256 devices in a mesh: ep: 16 (over y, x), tp: 16 (over z, core).
Axes of the slice: x: 4, y: 4, z: 8, core: 2. Of those that a mesh axis runs over, the one named last changes fastest.
Arguments:
- residual: bfloat16 [512, 2048], P('ep'), may hold values from -6 to 6
- mixer_gain: float32 [2048], replicated, may hold values from 0.1 to 1.9
- gate_proj: bfloat16 [2048, 2048], P('ep', 'tp'), may hold values from -0.125 to 0.125
- input_proj: bfloat16 [2048, 2048], P('ep', 'tp'), may hold values from -0.125 to 0.125
- write_proj: bfloat16 [2048, 2048], P('ep', 'tp'), may hold values from -0.125 to 0.125
- read_proj: bfloat16 [2048, 2048], P('ep', 'tp'), may hold values from -0.125 to 0.125
- step_proj: bfloat16 [2048, 32], replicated, may hold values from -0.125 to 0.125
- conv_weight: float32 [4, 3, 2048], replicated, may hold values from -3 to 3
- step_bias: float32 [32], replicated, may hold values from -4 to 0
- log_rate: float32 [32], replicated, may hold values from 0 to 2.5
- skip_gain: float32 [32], replicated, may hold values from -4 to 4
- group_gain: float32 [2048], replicated, may hold values from 0.1 to 1.9
- ssm_state: float32 [512, 32, 64, 128], P('ep', 'tp'), may hold values from -2 to 2
- conv_state: bfloat16 [512, 3, 3, 2048], P('ep', None, None, 'tp'), may hold values from -6 to 6
- out_proj: bfloat16 [2048, 2048], P('tp'), may hold values from -0.125 to 0.125
- ffn_gain: float32 [2048], replicated, may hold values from 0.1 to 1.9
- routes: int32 [512, 2], P('ep'), may hold values from 0 to 31, all different within a row; in each aligned block of 32 rows (0 to 31, 32 to 63, ...) at most 4 rows name the same one
- route_weight: float32 [512, 2], P('ep'), may hold values from 0.2 to 1
- expert_gate: bfloat16 [32, 2048, 2048], P('ep', None, 'tp'), may hold values from -0.125 to 0.125
- expert_up: bfloat16 [32, 2048, 2048], P('ep', None, 'tp'), may hold values from -0.125 to 0.125
- expert_down: bfloat16 [32, 2048, 2048], P('ep', 'tp'), may hold values from -0.125 to 0.125
- dense_gate: bfloat16 [2048, 2048], P(None, 'tp'), may hold values from -0.125 to 0.125
- dense_up: bfloat16 [2048, 2048], P(None, 'tp'), may hold values from -0.125 to 0.125
- dense_down: bfloat16 [2048, 2048], P('tp'), may hold values from -0.125 to 0.125
- blend_weight: bfloat16 [2048], replicated, may hold values from -0.125 to 0.125
Outputs:
- layer_out: bfloat16 [512, 2048], P('ep', 'tp')
- new_state: float32 [512, 32, 64, 128], P('ep', 'tp')
- new_conv: bfloat16 [512, 3, 3, 2048], P('ep', None, None, 'tp')
The draws below stay inside these ranges and needn't reach their ends.
Inputs may be any that keep to these rules, and one draw needn't show every extreme that they name: `routes`: each row names 2 different experts. Within the 32 rows of one index of ep no expert is named by more than 4 rows, and in some such block some expert is named by exactly 4 rows.
All inputs are finite; a program needn't handle non-finite values.
Results may differ from the reference program's by a relative error of at most 0.015.
Values may be sent and summed in bfloat16 or wider, within the bound.
A program may use at most 128 MiB of HBM per device.

```python
import math
import jax
import jax.numpy as jnp
import numpy as np
from jax import lax

D = 2048
HEADS = 32
HEAD_DIM = 64
GROUPS = 16
STATE = 128
KERNEL = 4
TOPK = 2
FFE = 2048
FFD = 2048
S_DEV = 32
D_INNER = 2048
EXPERTS = 32
TOK = 512
CAP = 4
N_EP = 16


def block_levels(stream_key, extent, pieces, smallest, high):
    loudness, own = 1.0, jax.random.fold_in(stream_key, 6)
    for position, shards_of in pieces:
        draws = jnp.exp(jax.random.uniform(jax.random.fold_in(own, position), (shards_of,), jnp.float32, smallest / len(pieces), high / len(pieces)))
        loudness = loudness * jnp.repeat(draws, extent[position] // shards_of).reshape([-1 if axis == position else 1 for axis in range(len(extent))])
    return loudness


def shared_out(key, own, number, rows, number_of, top, reach, lean):
    order = jax.random.permutation(key, number_of)
    heavy_load, ordinary = portions_of(number_of, rows * top, reach, lean, True), portions_of(number_of, rows * top, reach, lean, False)
    places = jnp.arange(number_of)

    def named(sizes, offset_by):
        used = int((sizes > 0).sum())
        fixed = max(1, used // 4)
        moved = fixed + (places - fixed + offset_by * (used - fixed)) % max(1, number_of - fixed)
        return jnp.zeros((number_of,), jnp.int32).at[order[jnp.where(places < fixed, places, moved)]].set(jnp.asarray(sizes, jnp.int32))

    sizes = jnp.where(number % 4 == 0, named(heavy_load, number // 4), named(ordinary, number - number // 4 - 1))
    mixed = jax.random.permutation(jax.random.fold_in(own, 3), number_of)
    giver, sink = mixed[0:number_of // 2 * 2:2], mixed[1:number_of // 2 * 2:2]
    margin = jnp.minimum(sizes[giver] - 1, reach - sizes[sink]) // 2
    margin = jnp.where((giver == order[0]) | (sink == order[0]) | (sizes[sink] == 0), 0, jnp.maximum(margin, 0))
    moved = jax.random.randint(jax.random.fold_in(own, 4), (number_of // 2,), 0, 1 << 20) % (margin + 1)
    sizes = sizes.at[giver].add(-moved).at[sink].add(moved)
    labels = jnp.searchsorted(jnp.cumsum(sizes), jnp.arange(rows * top), side="right").astype(jnp.int32)
    table = labels.reshape(top, rows).T
    table = table[jax.random.permutation(jax.random.fold_in(own, 1), rows)]
    offset_by = jax.random.randint(jax.random.fold_in(own, 2), (rows, 1), 0, top)
    return jnp.take_along_axis(table, (jnp.arange(top)[None, :] + offset_by) % top, axis=1)


def portions_of(amount, total, reach, skew, full):
    loads = [(1 << 20) // math.isqrt(rank ** skew) + 1 for rank in range(1, amount + 1)]
    largest = reach if full else min(reach, max(-(-total // amount), total * loads[0] // sum(loads)))
    least = 1 if total - largest >= amount - 1 else 0
    holding, surplus = [largest] + [least] * (amount - 1), total - largest - least * (amount - 1)
    while surplus > 0:
        candidates = [i for i in range(1, amount) if holding[i] < largest] or [i for i in range(1, amount) if holding[i] < reach]
        whole, left = sum([loads[i] for i in candidates]), surplus
        for i in candidates:
            more = min(reach - holding[i], max(1, left * loads[i] // whole), surplus)
            holding[i] = holding[i] + more
            surplus = surplus - more
    return np.array(holding)


def gaussian(key, dims, deviation, limit, cuts=(), held_as=jnp.bfloat16):
    values = deviation * jax.random.normal(key, dims, jnp.float32)
    if cuts:
        values = values * block_levels(key, dims, cuts, -0.22, 0.18)
    return jnp.clip(values, -limit, limit).astype(held_as)


def setup_inputs(seed: int = 0) -> dict:
    key_list = jax.random.split(jax.random.key(seed), 26)
    residual = gaussian(key_list[0], (TOK, D), 1.0, 6.0, ((0, 16),))
    mixer_gain = jnp.clip(1.0 + 0.18 * jax.random.normal(key_list[1], (D,), jnp.float32), 0.1, 1.9)
    gate_proj = gaussian(key_list[2], (D, D_INNER), D ** -0.5, 0.125, ((0, 16), (1, 16)))
    input_proj = gaussian(key_list[3], (D, D_INNER), D ** -0.5, 0.125, ((0, 16), (1, 16)))
    write_proj = gaussian(key_list[4], (D, D_INNER), D ** -0.5, 0.125, ((0, 16), (1, 16)))
    read_proj = gaussian(key_list[5], (D, D_INNER), D ** -0.5, 0.125, ((0, 16), (1, 16)))
    step_proj = gaussian(key_list[6], (D, HEADS), D ** -0.5, 0.125)
    conv_weight = gaussian(key_list[7], (KERNEL, 3, D_INNER), 0.5, 3.0, (), jnp.float32)
    step_bias = jnp.clip(jax.random.uniform(key_list[8], (HEADS,), jnp.float32, -4.0, 0.0), -4.0, 0.0)
    log_rate = jnp.clip(jax.random.uniform(key_list[9], (HEADS,), jnp.float32, 0.0, 2.5), 0.0, 2.5)
    skip_gain = gaussian(key_list[10], (HEADS,), 1.0, 4.0, (), jnp.float32)
    group_gain = jnp.clip(1.0 + 0.18 * jax.random.normal(key_list[11], (D_INNER,), jnp.float32), 0.1, 1.9)
    ssm_state = gaussian(key_list[12], (TOK, HEADS, HEAD_DIM, STATE), 0.3, 2.0, ((0, 16), (1, 16)), jnp.float32)
    conv_state = gaussian(key_list[13], (TOK, KERNEL - 1, 3, D_INNER), 1.0, 6.0, ((0, 16), (3, 16)))
    out_proj = gaussian(key_list[14], (D_INNER, D), D_INNER ** -0.5, 0.125, ((0, 16),))
    ffn_gain = jnp.clip(1.0 + 0.18 * jax.random.normal(key_list[15], (D,), jnp.float32), 0.1, 1.9)
    routes_keys = jax.random.split(jax.random.fold_in(key_list[16], 1), TOK // S_DEV)
    routes_turns = jax.random.permutation(jax.random.fold_in(key_list[16], 3), TOK // S_DEV)
    routes = jax.vmap(lambda own, number: shared_out(jax.random.fold_in(key_list[16], 2), own, number, S_DEV, EXPERTS, TOPK, CAP, 2))(routes_keys, routes_turns).reshape((TOK, TOPK))
    route_weight = jnp.clip(0.2 + 0.8 * jax.random.uniform(key_list[17], (TOK, TOPK), jnp.float32) ** block_levels(key_list[17], (TOK, TOPK), ((0, 16),), -0.2, 0.2), 0.2, 1.0)
    expert_gate = gaussian(key_list[18], (EXPERTS, D, FFE), D ** -0.5, 0.125, ((0, 16), (2, 16)))
    expert_up = gaussian(key_list[19], (EXPERTS, D, FFE), D ** -0.5, 0.125, ((0, 16), (2, 16)))
    expert_down = gaussian(key_list[20], (EXPERTS, FFE, D), FFE ** -0.5, 0.125, ((0, 16), (1, 16)))
    dense_gate = gaussian(key_list[21], (D, FFD), D ** -0.5, 0.125, ((1, 16),))
    dense_up = gaussian(key_list[22], (D, FFD), D ** -0.5, 0.125, ((1, 16),))
    dense_down = gaussian(key_list[23], (FFD, D), FFD ** -0.5, 0.125, ((0, 16),))
    blend_weight = gaussian(key_list[24], (D,), D ** -0.5, 0.125)
    return {"residual": residual, "mixer_gain": mixer_gain, "gate_proj": gate_proj, "input_proj": input_proj, "write_proj": write_proj, "read_proj": read_proj, "step_proj": step_proj, "conv_weight": conv_weight, "step_bias": step_bias, "log_rate": log_rate, "skip_gain": skip_gain, "group_gain": group_gain, "ssm_state": ssm_state, "conv_state": conv_state, "out_proj": out_proj, "ffn_gain": ffn_gain, "routes": routes, "route_weight": route_weight, "expert_gate": expert_gate, "expert_up": expert_up, "expert_down": expert_down, "dense_gate": dense_gate, "dense_up": dense_up, "dense_down": dense_down, "blend_weight": blend_weight}


epsilon = 1e-06

def rms_rows(values, gain_vector):
    floats_in = values.astype(jnp.float32)
    return floats_in * lax.rsqrt(lax.optimization_barrier(jnp.mean(floats_in * floats_in, axis=-1, keepdims=True)) + epsilon) * gain_vector

def reference(residual, mixer_gain, gate_proj, input_proj, write_proj, read_proj, step_proj, conv_weight, step_bias, log_rate, skip_gain, group_gain, ssm_state, conv_state, out_proj, ffn_gain, routes, route_weight, expert_gate, expert_up, expert_down, dense_gate, dense_up, dense_down, blend_weight):
    normed = rms_rows(residual, mixer_gain).astype(jnp.bfloat16)
    z_proj = jnp.dot(normed, gate_proj, preferred_element_type=jnp.float32).astype(jnp.bfloat16)
    x_proj = jnp.dot(normed, input_proj, preferred_element_type=jnp.float32).astype(jnp.bfloat16)
    b_proj = jnp.dot(normed, write_proj, preferred_element_type=jnp.float32).astype(jnp.bfloat16)
    c_proj = jnp.dot(normed, read_proj, preferred_element_type=jnp.float32).astype(jnp.bfloat16)
    step_raw = jnp.dot(normed, step_proj, preferred_element_type=jnp.float32)
    newest = jnp.stack((x_proj, b_proj, c_proj), axis=1)[:, None]
    stacked = jnp.concatenate((conv_state, newest), axis=1)
    new_conv = stacked[:, 1:]
    activated = jax.nn.silu(jnp.einsum('skcw,kcw->scw', stacked.astype(jnp.float32), conv_weight.astype(jnp.float32)))
    per_group = HEADS // GROUPS
    x_act = activated[:, 0].reshape(TOK, HEADS, HEAD_DIM)
    b_act = jnp.repeat(activated[:, 1].reshape(TOK, GROUPS, STATE), per_group, axis=1)
    c_act = jnp.repeat(activated[:, 2].reshape(TOK, GROUPS, STATE), per_group, axis=1)
    step_size = jax.nn.softplus(step_raw + step_bias)
    decay_factor = jnp.exp(-jnp.exp(log_rate) * step_size)
    new_state = decay_factor[:, :, None, None] * ssm_state + (step_size[:, :, None] * x_act)[..., None] * b_act[:, :, None, :]
    ssm_out = jnp.einsum('shpn,shn->shp', new_state, c_act) + skip_gain[None, :, None] * x_act
    gated_out = ssm_out.reshape(TOK, D_INNER) * jax.nn.silu(z_proj.astype(jnp.float32))
    grouped = gated_out.reshape(TOK, GROUPS, D_INNER // GROUPS)
    grouped = grouped * lax.rsqrt(lax.optimization_barrier(jnp.mean(grouped * grouped, axis=-1, keepdims=True)) + epsilon)
    mixed_out = (grouped.reshape(TOK, D_INNER) * group_gain).astype(jnp.bfloat16)
    resid_mid = (residual.astype(jnp.float32) + jnp.dot(mixed_out, out_proj, preferred_element_type=jnp.float32)).astype(jnp.bfloat16)
    normed_ffn = rms_rows(resid_mid, ffn_gain).astype(jnp.bfloat16)
    flat_routes = routes.reshape(N_EP, S_DEV * TOPK)
    onehot = (flat_routes[..., None] == jnp.arange(EXPERTS, dtype=jnp.int32)).astype(jnp.int32)
    slot_rank = lax.optimization_barrier(jnp.sum((jnp.cumsum(onehot, axis=1) - onehot) * onehot, axis=2)).astype(jnp.int32)
    source = jnp.broadcast_to(jnp.arange(N_EP, dtype=jnp.int32)[:, None], flat_routes.shape)
    repeated = jnp.repeat(normed_ffn, TOPK, axis=0).reshape(N_EP, S_DEV * TOPK, D)
    buffer = jnp.zeros((EXPERTS, N_EP, CAP, D), jnp.bfloat16).at[flat_routes, source, slot_rank].set(repeated)

    def expert(expert_args):
        expert_rows, w_gate, w_up, w_down = expert_args
        expert_rows = expert_rows.reshape(N_EP * CAP, D).astype(jnp.float32)
        gate_val = jnp.dot(expert_rows, w_gate.astype(jnp.float32))
        up_val = jnp.dot(expert_rows, w_up.astype(jnp.float32))
        hidden = (jax.nn.silu(gate_val) * up_val).astype(jnp.bfloat16)
        result = jnp.dot(hidden.astype(jnp.float32), w_down.astype(jnp.float32)).astype(jnp.bfloat16)
        return result.reshape(N_EP, CAP, D)
    results = lax.map(expert, (buffer, expert_gate, expert_up, expert_down))
    picked = results[flat_routes, source, slot_rank].astype(jnp.float32).reshape(TOK, TOPK, D)
    expert_mix = lax.optimization_barrier(jnp.sum(picked * route_weight[..., None], axis=1))
    gate_val = jnp.dot(normed_ffn, dense_gate, preferred_element_type=jnp.float32)
    up_val = jnp.dot(normed_ffn, dense_up, preferred_element_type=jnp.float32)
    dense_hidden = (jax.nn.silu(gate_val) * up_val).astype(jnp.bfloat16)
    dense_out = jnp.dot(dense_hidden, dense_down, preferred_element_type=jnp.float32)
    mix_weight = jax.nn.sigmoid(jnp.dot(normed_ffn, blend_weight, preferred_element_type=jnp.float32))
    layer_out = (resid_mid.astype(jnp.float32) + expert_mix + mix_weight[:, None] * dense_out).astype(jnp.bfloat16)
    return (layer_out, new_state, new_conv)
```

```python
import functools

import jax
import jax.numpy as jnp
from jax import lax
from jax.experimental import pallas as pl
from jax.experimental.pallas import tpu as pltpu
from jax.sharding import PartitionSpec as P

MESH = pl.DeviceIdType.MESH
F32 = jnp.float32
BF16 = jnp.bfloat16
EPS = 1e-06
ANY = pl.BlockSpec(memory_space=pl.ANY)
SMEM = pl.BlockSpec(memory_space=pltpu.SMEM)


def dot(a, b, dims=(((1,), (0,)), ((), ()))):
    return lax.dot_general(a, b, dims, preferred_element_type=F32)


def silu(v):
    return v * jax.nn.sigmoid(v)


def lanes(t):
    return slice(t * 128, (t + 1) * 128)


def kernel(
    residual,
    mixer_gain,
    gate_proj,
    input_proj,
    write_proj,
    read_proj,
    step_proj,
    conv_weight,
    step_bias,
    log_rate,
    skip_gain,
    group_gain,
    ssm_state,
    conv_state,
    out_proj,
    ffn_gain,
    routes,
    route_weight,
    expert_gate,
    expert_up,
    expert_down,
    dense_gate,
    dense_up,
    dense_down,
    blend_weight,
    layer_out,
    new_state,
    newest,
    res,
    mgain,
    ggain,
    fgain,
    blend,
    cw,
    sproj,
    rts,
    rw,
    cst,
    st,
    wp,
    wq,
    op,
    gu,
    dn,
    dgu,
    ddn,
    nat,
    np_,
    nq,
    rp,
    rq,
    sp,
    sq,
    r2p,
    r2q,
    dec,
    dxs,
    bs,
    cs,
    ys,
    nw,
    mixer_half,
    mixer_own,
    mixer_pair,
    rs_out,
    rs_in,
    rm,
    rmf_own,
    place,
    outb,
    rx,
    xn,
    half_e,
    own_e,
    pair_e,
    ret,
    back,
    xd,
    half_d,
    own_d,
    pair_d,
    rs2_out,
    rs2_in,
    lout,
    load_sem,
    store_sem,
    s1,
    r1,
    s2,
    r2,
    sz,
    rz,
    spair,
    rpair,
    sg,
    rg,
    sf,
    rf,
    sr,
    rr,
):
    E = lax.axis_index("ep")
    T = lax.axis_index("tp")
    Y, X = lax.div(E, 4), lax.rem(E, 4)
    Z, C = lax.div(T, 2), lax.rem(T, 2)
    pair = Z * 2 + (1 - C)

    def ep_at(d):
        dy, dx = lax.div(d, 4), lax.rem(d, 4)
        return lax.rem(Y + dy, 4) * 4 + lax.rem(X + dx, 4)

    def ep_from(d):
        dy, dx = lax.div(d, 4), lax.rem(d, 4)
        return lax.rem(Y + 4 - dy, 4) * 4 + lax.rem(X + 4 - dx, 4)

    def tp_at(d):
        return lax.rem(Z + d, 8) * 2 + C

    def loop(lo, hi, fn):
        lax.fori_loop(lo, hi, lambda i, c: (fn(i), c)[1], 0)

    def send(src, dst, ssem, rsem, ep, tp):
        return pltpu.make_async_remote_copy(
            src_ref=src,
            dst_ref=dst,
            send_sem=ssem,
            recv_sem=rsem,
            device_id={"ep": ep, "tp": tp},
            device_id_type=MESH,
        )

    bar = pltpu.get_barrier_semaphore()
    loop(
        1,
        16,
        lambda d: pl.semaphore_signal(
            bar, inc=1, device_id={"ep": ep_at(d), "tp": T}, device_id_type=MESH
        ),
    )
    loop(
        1,
        8,
        lambda d: pl.semaphore_signal(
            bar, inc=1, device_id={"ep": E, "tp": tp_at(d)}, device_id_type=MESH
        ),
    )
    pl.semaphore_signal(bar, inc=1, device_id={"ep": E, "tp": pair}, device_id_type=MESH)

    chan = pl.ds(pl.multiple_of(T * 128, 128), 128)
    loads = {}

    def load(name, *pairs):
        first = sum(len(v) for v in loads.values())
        copies = [
            pltpu.make_async_copy(s, d, load_sem.at[first + i]) for i, (s, d) in enumerate(pairs)
        ]
        for c in copies:
            c.start()
        loads[name] = copies

    def loaded(*names):
        for name in names:
            for c in loads[name]:
                c.wait()

    load("res", (residual, res), (mixer_gain, mgain))
    load(
        "proj",
        (gate_proj, wp.at[X, :, pl.ds(0, 128)]),
        (input_proj, wp.at[X, :, pl.ds(128, 128)]),
        (write_proj, wq.at[Y, :, pl.ds(0, 128)]),
        (read_proj, wq.at[Y, :, pl.ds(128, 128)]),
    )
    load(
        "small",
        (step_proj, sproj),
        (conv_weight.at[:, :, chan], cw),
        (conv_state, cst),
        (routes, rts),
        (route_weight, rw),
    )
    load("state", (ssm_state, st))
    load("op", (out_proj, op), (group_gain, ggain))
    load("ffn", (ffn_gain, fgain), (blend_weight, blend))
    load(
        "dense",
        (dense_gate, dgu.at[:, pl.ds(0, 128)]),
        (dense_up, dgu.at[:, pl.ds(128, 128)]),
        (dense_down, ddn),
    )
    load(
        "experts",
        (expert_gate, gu.at[:, :, pl.ds(0, 128)]),
        (expert_up, gu.at[:, :, pl.ds(128, 128)]),
        (expert_down, dn),
    )

    loaded("res")
    rv = res[...].astype(F32)
    scale = lax.rsqrt(jnp.mean(rv * rv, axis=-1, keepdims=True) + EPS)
    for t in range(16):
        blk = (rv[:, lanes(t)] * scale * mgain[t : t + 1, :]).astype(BF16)
        nat[:, lanes(t)] = blk
        np_[t // 4, :, lanes(t % 4)] = blk
        nq[t % 4, :, lanes(t // 4)] = blk
    rp[0] = np_[Y]
    rq[0] = nq[X]

    loaded("proj")
    pl.semaphore_wait(bar, 23)

    def y_at(d):
        return lax.rem(Y + d, 4) * 4 + X

    def x_at(d):
        return Y * 4 + lax.rem(X + d, 4)

    def w_p(d):
        return send(wp.at[X], wp.at[X], s1.at[d - 1], r1.at[d - 1], x_at(d), T)

    def w_q(d):
        return send(wq.at[Y], wq.at[Y], s1.at[d + 2], r1.at[d + 2], y_at(d), T)

    def n_p(d):
        return send(
            np_.at[lax.rem(Y + d, 4)], rp.at[d], s1.at[d + 5], r1.at[d + 5], y_at(d), T
        )

    def n_q(d):
        return send(
            nq.at[lax.rem(X + d, 4)], rq.at[d], s1.at[d + 8], r1.at[d + 8], x_at(d), T
        )

    for f in (w_p, w_q, n_p, n_q):
        loop(1, 4, lambda d, f=f: f(d).start())

    loaded("small")
    raw = dot(nat[...], sproj[...], (((1,), (1,)), ((), ())))
    lane32 = lax.broadcasted_iota(jnp.int32, (32, 32), 1)
    lane128 = lax.broadcasted_iota(jnp.int32, (32, 128), 1)
    dts = []
    for h in range(2):
        col = jnp.sum(jnp.where(lane32 == 2 * T + h, raw, 0.0), axis=1, keepdims=True)
        v = jnp.broadcast_to(col, (32, 128)) + step_bias[2 * T + h]
        dt = jnp.maximum(v, 0.0) + jnp.log1p(jnp.exp(-jnp.abs(v)))
        rate = jnp.exp(jnp.full((32, 128), log_rate[2 * T + h], F32))
        dec[h] = jnp.exp(-rate * dt)
        dts.append(dt)
    dt = jnp.where(lane128 < 64, dts[0], dts[1])
    skip = jnp.where(
        lane128 < 64,
        jnp.full((32, 128), skip_gain[2 * T], F32),
        jnp.full((32, 128), skip_gain[2 * T + 1], F32),
    )
    held = []
    for c in range(3):
        acc = cst[0, c].astype(F32) * cw[c, 0:1, :]
        for k in range(1, 3):
            acc = acc + cst[k, c].astype(F32) * cw[c, k : k + 1, :]
        held.append(acc)

    sub32 = lax.broadcasted_iota(jnp.int32, (32, 32), 0)
    hot = [(sub32 == rts[k : k + 1, :]).astype(F32) for k in range(2)]
    before = (sub32 < lane32).astype(BF16)
    prefix = dot((hot[0] + hot[1]).astype(BF16), before)
    slot = lax.broadcasted_iota(jnp.int32, (128, 32), 0)
    spots = []
    for k in range(2):
        rank = jnp.sum(hot[k] * prefix, axis=0, keepdims=True).astype(jnp.int32)
        spots.append((slot == rts[k : k + 1, :] * 4 + rank).astype(F32))
    place[0] = spots[0] + spots[1]
    place[1] = spots[0] * rw[0:1, :] + spots[1] * rw[1:2, :]

    loop(1, 4, lambda d: w_p(d).wait_recv())
    loop(1, 4, lambda d: n_p(d).wait_recv())
    part_p = dot(rp[...].reshape(128, 512), wp[...].reshape(512, 256))
    sp[...] = part_p.astype(BF16).reshape(4, 32, 256)

    def back_p(d):
        return send(
            sp.at[d], r2p.at[d - 1], s2.at[d - 1], r2.at[d - 1], y_at(4 - d), T
        )

    loop(1, 4, lambda d: back_p(d).start())
    loop(1, 4, lambda d: w_q(d).wait_recv())
    loop(1, 4, lambda d: n_q(d).wait_recv())
    part_q = dot(rq[...].reshape(128, 512), wq[...].reshape(512, 256))
    sq[...] = part_q.astype(BF16).reshape(4, 32, 256)

    def back_q(d):
        return send(
            sq.at[d], r2q.at[d - 1], s2.at[d + 2], r2.at[d + 2], x_at(4 - d), T
        )

    loop(1, 4, lambda d: back_q(d).start())
    own_p, own_q = part_p[0:32], part_q[0:32]
    loaded("state", "op")
    loop(1, 4, lambda d: back_p(d).wait_recv())
    for d in range(3):
        own_p = own_p + r2p[d].astype(F32)
    loop(1, 4, lambda d: back_q(d).wait_recv())
    for d in range(3):
        own_q = own_q + r2q[d].astype(F32)
    z_proj = own_p[:, 0:128].astype(BF16).astype(F32)
    fresh = [own_p[:, 128:256], own_q[:, 0:128], own_q[:, 128:256]]
    acts = []
    for c in range(3):
        row = fresh[c].astype(BF16)
        nw[c] = row
        acts.append(silu(held[c] + row.astype(F32) * cw[c, 3:4, :]))
    x_act = acts[0]
    dxs[...] = dt * x_act
    bs[...] = acts[1]
    cs[...] = acts[2]

    lane_y = lax.broadcasted_iota(jnp.int32, (64, 128), 1)

    def tokens(g):
        base = pl.multiple_of(g * 8, 8)
        dx_t = jnp.transpose(dxs[pl.ds(base, 8), :])
        yt = [jnp.zeros((64, 128), F32), jnp.zeros((64, 128), F32)]
        for i in range(8):
            s = base + i
            b_row = bs[pl.ds(s, 1), :]
            c_row = cs[pl.ds(s, 1), :]
            for h in range(2):
                ns = dec[h, pl.ds(s, 1), :] * st[s, h] + dx_t[h * 64 : h * 64 + 64, i : i + 1] * b_row
                st[s, h] = ns
                y = jnp.sum(ns * c_row, axis=1, keepdims=True)
                yt[h] = jnp.where(lane_y == i, y, yt[h])
        ys[pl.ds(base, 8), :] = jnp.transpose(jnp.concatenate(yt, axis=0))[0:8]

    loop(0, 4, tokens)
    keep_state = pltpu.make_async_copy(st, new_state, store_sem.at[0])
    keep_conv = pltpu.make_async_copy(nw, newest, store_sem.at[1])

    gated = (ys[...] + skip * x_act) * silu(z_proj)
    gated = gated * lax.rsqrt(jnp.mean(gated * gated, axis=-1, keepdims=True) + EPS)
    mixed = (gated * ggain[pl.ds(T, 1), :]).astype(BF16)
    part = dot(mixed, op[...])
    for t in range(16):
        mixer_half[t % 2, t // 2] = part[:, lanes(t)].astype(BF16)
        if t % 2 == 0:
            mixer_own[t // 2] = jnp.where(C == 0, part[:, lanes(t)], part[:, lanes(t + 1)])

    def to_pair(src, dst, i):
        return send(src, dst, spair.at[i], rpair.at[i], E, pair)

    swap_mixer = to_pair(mixer_half.at[1 - C], mixer_pair, 0)
    swap_mixer.start()
    keep_state.start()
    keep_conv.start()
    swap_mixer.wait_recv()
    mixer_own[...] = mixer_own[...] + mixer_pair[...].astype(F32)
    rs_out[...] = mixer_own[...].astype(BF16)

    def z_block(d):
        return lax.rem(Z + d, 8)

    def scatter(d):
        return send(
            rs_out.at[z_block(d)], rs_in.at[d - 1], sz.at[d - 1], rz.at[d - 1], E, tp_at(d)
        )

    loop(1, 8, lambda d: scatter(d).start())
    total = mixer_own[Z]
    resid_cols = res[:, chan].astype(F32)
    loop(1, 8, lambda d: scatter(d).wait_recv())
    for d in range(7):
        total = total + rs_in[d].astype(F32)
    rm[C, Z] = (resid_cols + total).astype(BF16)

    def gather(d):
        return send(
            rm.at[C, Z], rm.at[C, Z], sz.at[d + 6], rz.at[d + 6], E, tp_at(d)
        )

    def gather_in(d):
        return send(
            rm.at[C, z_block(8 - d)], rm.at[C, z_block(8 - d)], sz.at[d + 6], rz.at[d + 6], E, tp_at(d)
        )

    loop(1, 8, lambda d: gather(d).start())
    loaded("dense", "experts", "ffn")
    loop(1, 8, lambda d: gather_in(d).wait_recv())
    swap_resid = to_pair(rm.at[C], rm.at[C], 1)
    swap_resid.start()

    mine = rm[C]
    mine = jnp.concatenate([mine[z] for z in range(8)], axis=1)
    rows = dot(place[0].astype(BF16), mine).reshape(16, 8, 1024)
    outb[...] = jnp.concatenate([rows[:, :, :512], rows[:, :, 512:]], axis=1).astype(BF16)
    rx[C, 0] = outb[E]

    def dispatch(d):
        return send(outb.at[ep_at(d)], rx.at[C, d], sg.at[d - 1], rg.at[d - 1], ep_at(d), T)

    def forward(d):
        return send(rx.at[C, d], rx.at[C, d], sf.at[d], rf.at[d], E, pair)

    def forward_in(d):
        return send(rx.at[1 - C, d], rx.at[1 - C, d], sf.at[d], rf.at[d], E, pair)

    loop(1, 16, lambda d: dispatch(d).start())
    forward(0).start()

    to_pair(rm.at[1 - C], rm.at[1 - C], 1).wait_recv()
    ms = jnp.zeros((32, 1), F32)
    for t in range(16):
        v = rm[t % 2, t // 2].astype(F32)
        ms = ms + jnp.sum(v * v, axis=1, keepdims=True)
    scale = lax.rsqrt(ms * (1.0 / 2048) + EPS)
    logit = jnp.zeros((32, 128), F32)
    for t in range(16):
        v = rm[t % 2, t // 2].astype(F32)
        n = (v * scale * fgain[t : t + 1, :]).astype(BF16)
        xd[:, lanes(t)] = n
        logit = logit + n.astype(F32) * blend[t : t + 1, :].astype(F32)
    mix_weight = jax.nn.sigmoid(jnp.sum(logit, axis=1, keepdims=True))
    hid = dot(xd[...], dgu[...])
    hid = (silu(hid[:, 0:128]) * hid[:, 128:256]).astype(BF16)
    part = dot(hid, ddn[...]) * mix_weight
    for t in range(16):
        half_d[t % 2, t // 2] = part[:, lanes(t)].astype(BF16)
        if t % 2 == 0:
            own_d[t // 2] = jnp.where(C == 0, part[:, lanes(t)], part[:, lanes(t + 1)])
    swap_dense = to_pair(half_d.at[1 - C], pair_d, 2)
    swap_dense.start()

    def arrive(d):
        dispatch(d).wait_recv()
        forward(d).start()

    loop(1, 16, arrive)
    loop(0, 16, lambda d: forward_in(d).wait_recv())

    def side(c):
        v = rx[c].astype(F32).reshape(16, 2, 8, 512)
        return v[:, 0].reshape(128, 512), v[:, 1].reshape(128, 512)

    quarters = [side(0), side(1)]
    ms = jnp.zeros((128, 1), F32)
    for q in quarters:
        for v in q:
            ms = ms + jnp.sum(v * v, axis=1, keepdims=True)
    scale = lax.rsqrt(ms * (1.0 / 2048) + EPS)
    for t in range(16):
        zz = t // 2
        v = quarters[t % 2][zz // 4][:, lanes(zz % 4)]
        xn[:, lanes(t)] = (v * scale * fgain[t : t + 1, :]).astype(BF16)
    row = lax.broadcasted_iota(jnp.int32, (128, 128), 0)
    hids = []
    for j in range(2):
        hid = dot(xn[...], gu[j])
        hid = silu(hid[:, 0:128]) * hid[:, 128:256]
        mine = (row % 8 >= 4) if j else (row % 8 < 4)
        hids.append(jnp.where(mine, hid, 0.0).astype(BF16))
    part = dot(jnp.concatenate(hids, axis=1), dn[...].reshape(256, 2048))

    def folded(v):
        lo = v[0].reshape(16, 8, 512)
        hi = v[1].reshape(16, 8, 512)
        return jnp.concatenate([lo, hi], axis=1)

    for q in range(2):
        even = jnp.concatenate([part[:, lanes(2 * z)] for z in range(4 * q, 4 * q + 4)], axis=1)
        odd = jnp.concatenate([part[:, lanes(2 * z + 1)] for z in range(4 * q, 4 * q + 4)], axis=1)
        half_e[0, q] = even.astype(BF16)
        half_e[1, q] = odd.astype(BF16)
        own_e[q] = jnp.where(C == 0, even, odd)
    swap_expert = to_pair(half_e.at[1 - C], pair_e, 3)
    swap_expert.start()
    swap_expert.wait_recv()
    both = own_e[...] + pair_e[...].astype(F32)
    ret[...] = folded(both).astype(BF16)
    back[E] = ret[0]

    def give_back(d):
        return send(ret.at[d], back.at[E], sr.at[d - 1], rr.at[d - 1], ep_from(d), T)

    def give_back_in(d):
        return send(ret.at[d], back.at[ep_at(d)], sr.at[d - 1], rr.at[d - 1], ep_from(d), T)

    loop(1, 16, lambda d: give_back(d).start())
    swap_dense.wait_recv()
    own_d[...] = own_d[...] + pair_d[...].astype(F32)
    weight = place[1]
    w_hi = weight.astype(BF16)
    w_lo = (weight - w_hi.astype(F32)).astype(BF16)
    loop(1, 16, lambda d: give_back_in(d).wait_recv())
    v = back[...].astype(F32).reshape(16, 2, 8, 512)
    first = (((0,), (0,)), ((), ()))
    for q in range(2):
        rows = v[:, q].reshape(128, 512).astype(BF16)
        mix = dot(w_hi, rows, first) + dot(w_lo, rows, first)
        for z in range(4):
            own_d[4 * q + z] = own_d[4 * q + z] + mix[:, lanes(z)]
    rs2_out[...] = own_d[...].astype(BF16)

    def scatter2(d):
        return send(
            rs2_out.at[z_block(d)], rs2_in.at[d - 1], sz.at[d + 13], rz.at[d + 13], E, tp_at(d)
        )

    loop(1, 8, lambda d: scatter2(d).start())
    total = own_d[Z] + rm[C, Z].astype(F32)
    loop(1, 8, lambda d: scatter2(d).wait_recv())
    for d in range(7):
        total = total + rs2_in[d].astype(F32)
    lout[...] = total.astype(BF16)
    done = pltpu.make_async_copy(lout, layer_out, store_sem.at[2])
    done.start()

    for f in (w_p, w_q, n_p, n_q, back_p, back_q):
        loop(1, 4, lambda d, f=f: f(d).wait_send())
    for f in (scatter, gather, scatter2):
        loop(1, 8, lambda d, f=f: f(d).wait_send())
    for f in (dispatch, give_back):
        loop(1, 16, lambda d, f=f: f(d).wait_send())
    loop(0, 16, lambda d: forward(d).wait_send())
    for s in (swap_mixer, swap_resid, swap_dense, swap_expert):
        s.wait_send()
    keep_state.wait()
    keep_conv.wait()
    done.wait()


SCRATCH = [
    ((32, 2048), BF16),
    ((16, 128), F32),
    ((16, 128), F32),
    ((16, 128), F32),
    ((16, 128), BF16),
    ((3, 4, 128), F32),
    ((32, 2048), BF16),
    ((2, 32), jnp.int32),
    ((2, 32), F32),
    ((3, 3, 32, 128), BF16),
    ((32, 2, 64, 128), F32),
    ((4, 128, 256), BF16),
    ((4, 128, 256), BF16),
    ((128, 2048), BF16),
    ((2, 2048, 256), BF16),
    ((2, 128, 2048), BF16),
    ((2048, 256), BF16),
    ((128, 2048), BF16),
    ((32, 2048), BF16),
    ((4, 32, 512), BF16),
    ((4, 32, 512), BF16),
    ((4, 32, 512), BF16),
    ((4, 32, 512), BF16),
    ((4, 32, 256), BF16),
    ((4, 32, 256), BF16),
    ((3, 32, 256), BF16),
    ((3, 32, 256), BF16),
    ((2, 32, 128), F32),
    ((32, 128), F32),
    ((32, 128), F32),
    ((32, 128), F32),
    ((32, 128), F32),
    ((3, 32, 128), BF16),
    ((2, 8, 32, 128), BF16),
    ((8, 32, 128), F32),
    ((8, 32, 128), BF16),
    ((8, 32, 128), BF16),
    ((7, 32, 128), BF16),
    ((2, 8, 32, 128), BF16),
    ((8, 128), F32),
    ((2, 128, 32), F32),
    ((16, 16, 512), BF16),
    ((2, 16, 16, 512), BF16),
    ((128, 2048), BF16),
    ((2, 2, 128, 512), BF16),
    ((2, 128, 512), F32),
    ((2, 128, 512), BF16),
    ((16, 16, 512), BF16),
    ((16, 16, 512), BF16),
    ((32, 2048), BF16),
    ((2, 8, 32, 128), BF16),
    ((8, 32, 128), F32),
    ((8, 32, 128), BF16),
    ((8, 32, 128), BF16),
    ((7, 32, 128), BF16),
    ((32, 128), BF16),
]


def on_device(*args):
    (
        residual,
        mixer_gain,
        gate_proj,
        input_proj,
        write_proj,
        read_proj,
        step_proj,
        conv_weight,
        step_bias,
        log_rate,
        skip_gain,
        group_gain,
        ssm_state,
        conv_state,
        out_proj,
        ffn_gain,
        routes,
        route_weight,
        expert_gate,
        expert_up,
        expert_down,
        dense_gate,
        dense_up,
        dense_down,
        blend_weight,
    ) = args
    conv_t = jnp.transpose(conv_state, (1, 2, 0, 3))
    layer_out, new_state, newest = pl.pallas_call(
        kernel,
        out_shape=(
            jax.ShapeDtypeStruct((32, 128), BF16),
            jax.ShapeDtypeStruct((32, 2, 64, 128), F32),
            jax.ShapeDtypeStruct((3, 32, 128), BF16),
        ),
        in_specs=[ANY] * 8 + [SMEM] * 3 + [ANY] * 14,
        out_specs=(ANY, ANY, ANY),
        scratch_shapes=[pltpu.VMEM(s, d) for s, d in SCRATCH]
        + [
            pltpu.SemaphoreType.DMA((24,)),
            pltpu.SemaphoreType.DMA((3,)),
            pltpu.SemaphoreType.DMA((12,)),
            pltpu.SemaphoreType.DMA((12,)),
            pltpu.SemaphoreType.DMA((6,)),
            pltpu.SemaphoreType.DMA((6,)),
            pltpu.SemaphoreType.DMA((21,)),
            pltpu.SemaphoreType.DMA((21,)),
            pltpu.SemaphoreType.DMA((4,)),
            pltpu.SemaphoreType.DMA((4,)),
            pltpu.SemaphoreType.DMA((15,)),
            pltpu.SemaphoreType.DMA((15,)),
            pltpu.SemaphoreType.DMA((16,)),
            pltpu.SemaphoreType.DMA((16,)),
            pltpu.SemaphoreType.DMA((15,)),
            pltpu.SemaphoreType.DMA((15,)),
        ],
        compiler_params=pltpu.CompilerParams(
            collective_id=0, has_side_effects=True, vmem_limit_bytes=40 * 1024 * 1024
        ),
    )(
        residual,
        mixer_gain.reshape(16, 128),
        gate_proj,
        input_proj,
        write_proj,
        read_proj,
        step_proj.T,
        jnp.transpose(conv_weight, (1, 0, 2)),
        step_bias,
        log_rate,
        skip_gain,
        group_gain.reshape(16, 128),
        ssm_state,
        conv_t,
        out_proj,
        ffn_gain.reshape(16, 128),
        routes.T,
        route_weight.T,
        expert_gate,
        expert_up,
        expert_down,
        dense_gate,
        dense_up,
        dense_down,
        blend_weight.reshape(16, 128),
    )
    new_conv = jnp.concatenate([conv_t[1:], newest[None]], axis=0)
    return layer_out, new_state, jnp.transpose(new_conv, (2, 0, 1, 3))


def solution(mesh):
    return jax.shard_map(
        on_device,
        mesh=mesh,
        in_specs=(
            P("ep", None),
            P(),
            P("ep", "tp"),
            P("ep", "tp"),
            P("ep", "tp"),
            P("ep", "tp"),
            P(),
            P(),
            P(),
            P(),
            P(),
            P(),
            P("ep", "tp", None, None),
            P("ep", None, None, "tp"),
            P("tp", None),
            P(),
            P("ep", None),
            P("ep", None),
            P("ep", None, "tp"),
            P("ep", None, "tp"),
            P("ep", "tp", None),
            P(None, "tp"),
            P(None, "tp"),
            P("tp", None),
            P(),
        ),
        out_specs=(P("ep", "tp"), P("ep", "tp", None, None), P("ep", None, None, "tp")),
        check_vma=False,
    )
```

```python
import functools

import jax
import jax.numpy as jnp
from jax import lax
from jax.experimental import pallas as pl
from jax.experimental.pallas import tpu as pltpu
from jax.sharding import PartitionSpec as P

MESH = pl.DeviceIdType.MESH
F32 = jnp.float32
BF16 = jnp.bfloat16
EPS = 1e-06
ANY = pl.BlockSpec(memory_space=pl.ANY)
SMEM = pl.BlockSpec(memory_space=pltpu.SMEM)


def dot(a, b, dims=(((1,), (0,)), ((), ()))):
    return lax.dot_general(a, b, dims, preferred_element_type=F32)


def silu(v):
    return v * jax.nn.sigmoid(v)


def lanes(t):
    return slice(t * 128, (t + 1) * 128)


def kernel(
    residual,
    mixer_gain,
    gate_proj,
    input_proj,
    write_proj,
    read_proj,
    step_proj,
    conv_weight,
    step_bias,
    log_rate,
    skip_gain,
    group_gain,
    ssm_state,
    conv_state,
    out_proj,
    ffn_gain,
    routes,
    route_weight,
    expert_gate,
    expert_up,
    expert_down,
    dense_gate,
    dense_up,
    dense_down,
    blend_weight,
    layer_out,
    new_state,
    newest,
    res,
    mgain,
    ggain,
    fgain,
    blend,
    cw,
    sproj,
    rts,
    rw,
    cst,
    st,
    wp,
    wq,
    op,
    gu,
    dn,
    dgu,
    ddn,
    nat,
    np_,
    nq,
    rp,
    rq,
    sp,
    sq,
    r2p,
    r2q,
    dec,
    dxs,
    bs,
    cs,
    ys,
    nw,
    mixer_half,
    mixer_own,
    mixer_pair,
    rs_out,
    rs_in,
    rm,
    rmf_own,
    place,
    outb,
    rx,
    xn,
    half_e,
    own_e,
    pair_e,
    ret,
    back,
    xd,
    half_d,
    own_d,
    pair_d,
    rs2_out,
    rs2_in,
    lout,
    load_sem,
    store_sem,
    s1,
    r1,
    s2,
    r2,
    sz,
    rz,
    spair,
    rpair,
    sg,
    rg,
    sf,
    rf,
    sr,
    rr,
):
    E = lax.axis_index("ep")
    T = lax.axis_index("tp")
    Y, X = lax.div(E, 4), lax.rem(E, 4)
    Z, C = lax.div(T, 2), lax.rem(T, 2)
    pair = Z * 2 + (1 - C)

    def ep_at(d):
        dy, dx = lax.div(d, 4), lax.rem(d, 4)
        return lax.rem(Y + dy, 4) * 4 + lax.rem(X + dx, 4)

    def ep_from(d):
        dy, dx = lax.div(d, 4), lax.rem(d, 4)
        return lax.rem(Y + 4 - dy, 4) * 4 + lax.rem(X + 4 - dx, 4)

    def tp_at(d):
        return lax.rem(Z + d, 8) * 2 + C

    def loop(lo, hi, fn):
        lax.fori_loop(lo, hi, lambda i, c: (fn(i), c)[1], 0)

    def send(src, dst, ssem, rsem, ep, tp):
        return pltpu.make_async_remote_copy(
            src_ref=src,
            dst_ref=dst,
            send_sem=ssem,
            recv_sem=rsem,
            device_id={"ep": ep, "tp": tp},
            device_id_type=MESH,
        )

    bar = pltpu.get_barrier_semaphore()
    loop(
        1,
        16,
        lambda d: pl.semaphore_signal(
            bar, inc=1, device_id={"ep": ep_at(d), "tp": T}, device_id_type=MESH
        ),
    )
    loop(
        1,
        8,
        lambda d: pl.semaphore_signal(
            bar, inc=1, device_id={"ep": E, "tp": tp_at(d)}, device_id_type=MESH
        ),
    )
    pl.semaphore_signal(bar, inc=1, device_id={"ep": E, "tp": pair}, device_id_type=MESH)

    chan = pl.ds(pl.multiple_of(T * 128, 128), 128)
    loads = {}

    def load(name, *pairs):
        first = sum(len(v) for v in loads.values())
        copies = [
            pltpu.make_async_copy(s, d, load_sem.at[first + i]) for i, (s, d) in enumerate(pairs)
        ]
        for c in copies:
            c.start()
        loads[name] = copies

    def loaded(*names):
        for name in names:
            for c in loads[name]:
                c.wait()

    load("res", (residual, res), (mixer_gain, mgain))
    load(
        "proj",
        (gate_proj, wp.at[X, :, pl.ds(0, 128)]),
        (input_proj, wp.at[X, :, pl.ds(128, 128)]),
        (write_proj, wq.at[Y, :, pl.ds(0, 128)]),
        (read_proj, wq.at[Y, :, pl.ds(128, 128)]),
    )
    load(
        "small",
        (step_proj, sproj),
        (conv_weight.at[:, :, chan], cw),
        (conv_state, cst),
        (routes, rts),
        (route_weight, rw),
    )
    load("state", (ssm_state, st))
    load("op", (out_proj, op), (group_gain, ggain))
    load("ffn", (ffn_gain, fgain), (blend_weight, blend))
    load(
        "dense",
        (dense_gate, dgu.at[:, pl.ds(0, 128)]),
        (dense_up, dgu.at[:, pl.ds(128, 128)]),
        (dense_down, ddn),
    )
    load(
        "experts",
        (expert_gate, gu.at[:, :, pl.ds(0, 128)]),
        (expert_up, gu.at[:, :, pl.ds(128, 128)]),
        (expert_down, dn),
    )

    loaded("res")
    rv = res[...].astype(F32)
    scale = lax.rsqrt(jnp.mean(rv * rv, axis=-1, keepdims=True) + EPS)
    for t in range(16):
        blk = (rv[:, lanes(t)] * scale * mgain[t : t + 1, :]).astype(BF16)
        nat[:, lanes(t)] = blk
        np_[t // 4, :, lanes(t % 4)] = blk
        nq[t % 4, :, lanes(t // 4)] = blk
    rp[0] = np_[Y]
    rq[0] = nq[X]

    loaded("proj")
    pl.semaphore_wait(bar, 23)

    def y_at(d):
        return lax.rem(Y + d, 4) * 4 + X

    def x_at(d):
        return Y * 4 + lax.rem(X + d, 4)

    def w_p(d):
        return send(wp.at[X], wp.at[X], s1.at[d - 1], r1.at[d - 1], x_at(d), T)

    def w_q(d):
        return send(wq.at[Y], wq.at[Y], s1.at[d + 2], r1.at[d + 2], y_at(d), T)

    def n_p(d):
        return send(
            np_.at[lax.rem(Y + d, 4)], rp.at[d], s1.at[d + 5], r1.at[d + 5], y_at(d), T
        )

    def n_q(d):
        return send(
            nq.at[lax.rem(X + d, 4)], rq.at[d], s1.at[d + 8], r1.at[d + 8], x_at(d), T
        )

    for f in (w_p, w_q, n_p, n_q):
        loop(1, 4, lambda d, f=f: f(d).start())

    loaded("small")
    raw = dot(nat[...], sproj[...], (((1,), (1,)), ((), ())))
    lane32 = lax.broadcasted_iota(jnp.int32, (32, 32), 1)
    lane128 = lax.broadcasted_iota(jnp.int32, (32, 128), 1)
    dts = []
    for h in range(2):
        col = jnp.sum(jnp.where(lane32 == 2 * T + h, raw, 0.0), axis=1, keepdims=True)
        v = jnp.broadcast_to(col, (32, 128)) + step_bias[2 * T + h]
        dt = jnp.maximum(v, 0.0) + jnp.log1p(jnp.exp(-jnp.abs(v)))
        rate = jnp.exp(jnp.full((32, 128), log_rate[2 * T + h], F32))
        dec[h] = jnp.exp(-rate * dt)
        dts.append(dt)
    dt = jnp.where(lane128 < 64, dts[0], dts[1])
    skip = jnp.where(
        lane128 < 64,
        jnp.full((32, 128), skip_gain[2 * T], F32),
        jnp.full((32, 128), skip_gain[2 * T + 1], F32),
    )
    held = []
    for c in range(3):
        acc = cst[0, c].astype(F32) * cw[c, 0:1, :]
        for k in range(1, 3):
            acc = acc + cst[k, c].astype(F32) * cw[c, k : k + 1, :]
        held.append(acc)

    sub32 = lax.broadcasted_iota(jnp.int32, (32, 32), 0)
    hot = [(sub32 == rts[k : k + 1, :]).astype(F32) for k in range(2)]
    before = (sub32 < lane32).astype(BF16)
    prefix = dot((hot[0] + hot[1]).astype(BF16), before)
    slot = lax.broadcasted_iota(jnp.int32, (128, 32), 0)
    spots = []
    for k in range(2):
        rank = jnp.sum(hot[k] * prefix, axis=0, keepdims=True).astype(jnp.int32)
        spots.append((slot == rts[k : k + 1, :] * 4 + rank).astype(F32))
    place[0] = spots[0] + spots[1]
    place[1] = spots[0] * rw[0:1, :] + spots[1] * rw[1:2, :]

    loop(1, 4, lambda d: w_p(d).wait_recv())
    loop(1, 4, lambda d: n_p(d).wait_recv())
    part_p = dot(rp[...].reshape(128, 512), wp[...].reshape(512, 256))
    sp[...] = part_p.astype(BF16).reshape(4, 32, 256)

    def back_p(d):
        return send(
            sp.at[d], r2p.at[d - 1], s2.at[d - 1], r2.at[d - 1], y_at(4 - d), T
        )

    loop(1, 4, lambda d: back_p(d).start())
    loop(1, 4, lambda d: w_q(d).wait_recv())
    loop(1, 4, lambda d: n_q(d).wait_recv())
    part_q = dot(rq[...].reshape(128, 512), wq[...].reshape(512, 256))
    sq[...] = part_q.astype(BF16).reshape(4, 32, 256)

    def back_q(d):
        return send(
            sq.at[d], r2q.at[d - 1], s2.at[d + 2], r2.at[d + 2], x_at(4 - d), T
        )

    loop(1, 4, lambda d: back_q(d).start())
    own_p, own_q = part_p[0:32], part_q[0:32]
    loaded("state", "op")
    loop(1, 4, lambda d: back_p(d).wait_recv())
    for d in range(3):
        own_p = own_p + r2p[d].astype(F32)
    loop(1, 4, lambda d: back_q(d).wait_recv())
    for d in range(3):
        own_q = own_q + r2q[d].astype(F32)
    z_proj = own_p[:, 0:128].astype(BF16).astype(F32)
    fresh = [own_p[:, 128:256], own_q[:, 0:128], own_q[:, 128:256]]
    acts = []
    for c in range(3):
        row = fresh[c].astype(BF16)
        nw[c] = row
        acts.append(silu(held[c] + row.astype(F32) * cw[c, 3:4, :]))
    x_act = acts[0]
    dxs[...] = dt * x_act
    bs[...] = acts[1]
    cs[...] = acts[2]

    lane_y = lax.broadcasted_iota(jnp.int32, (64, 128), 1)

    def tokens(g):
        base = pl.multiple_of(g * 8, 8)
        dx_t = jnp.transpose(dxs[pl.ds(base, 8), :])
        yt = [jnp.zeros((64, 128), F32), jnp.zeros((64, 128), F32)]
        for i in range(8):
            s = base + i
            b_row = bs[pl.ds(s, 1), :]
            c_row = cs[pl.ds(s, 1), :]
            for h in range(2):
                ns = dec[h, pl.ds(s, 1), :] * st[s, h] + dx_t[h * 64 : h * 64 + 64, i : i + 1] * b_row
                st[s, h] = ns
                y = jnp.sum(ns * c_row, axis=1, keepdims=True)
                yt[h] = jnp.where(lane_y == i, y, yt[h])
        ys[pl.ds(base, 8), :] = jnp.transpose(jnp.concatenate(yt, axis=0))[0:8]

    loop(0, 4, tokens)
    keep_state = pltpu.make_async_copy(st, new_state, store_sem.at[0])
    keep_conv = pltpu.make_async_copy(nw, newest, store_sem.at[1])

    gated = (ys[...] + skip * x_act) * silu(z_proj)
    gated = gated * lax.rsqrt(jnp.mean(gated * gated, axis=-1, keepdims=True) + EPS)
    mixed = (gated * ggain[pl.ds(T, 1), :]).astype(BF16)
    part = dot(mixed, op[...])
    for t in range(16):
        mixer_half[t % 2, t // 2] = part[:, lanes(t)].astype(BF16)
        if t % 2 == 0:
            mixer_own[t // 2] = jnp.where(C == 0, part[:, lanes(t)], part[:, lanes(t + 1)])

    def to_pair(src, dst, i):
        return send(src, dst, spair.at[i], rpair.at[i], E, pair)

    swap_mixer = to_pair(mixer_half.at[1 - C], mixer_pair, 0)
    swap_mixer.start()
    keep_state.start()
    keep_conv.start()
    swap_mixer.wait_recv()
    mixer_own[...] = mixer_own[...] + mixer_pair[...].astype(F32)
    rs_out[...] = mixer_own[...].astype(BF16)

    def z_block(d):
        return lax.rem(Z + d, 8)

    def scatter(d):
        return send(
            rs_out.at[z_block(d)], rs_in.at[d - 1], sz.at[d - 1], rz.at[d - 1], E, tp_at(d)
        )

    loop(1, 8, lambda d: scatter(d).start())
    total = mixer_own[Z]
    resid_cols = res[:, chan].astype(F32)
    loop(1, 8, lambda d: scatter(d).wait_recv())
    for d in range(7):
        total = total + rs_in[d].astype(F32)
    rm[C, Z] = (resid_cols + total).astype(BF16)

    def gather(d):
        return send(
            rm.at[C, Z], rm.at[C, Z], sz.at[d + 6], rz.at[d + 6], E, tp_at(d)
        )

    def gather_in(d):
        return send(
            rm.at[C, z_block(8 - d)], rm.at[C, z_block(8 - d)], sz.at[d + 6], rz.at[d + 6], E, tp_at(d)
        )

    loop(1, 8, lambda d: gather(d).start())
    loaded("dense", "experts", "ffn")
    loop(1, 8, lambda d: gather_in(d).wait_recv())
    swap_resid = to_pair(rm.at[C], rm.at[C], 1)
    swap_resid.start()

    mine = rm[C]
    mine = jnp.concatenate([mine[z] for z in range(8)], axis=1)
    rows = dot(place[0].astype(BF16), mine).reshape(16, 8, 1024)
    outb[...] = jnp.concatenate([rows[:, :, :512], rows[:, :, 512:]], axis=1).astype(BF16)
    rx[C, 0] = outb[E]

    def dispatch(d):
        return send(outb.at[ep_at(d)], rx.at[C, d], sg.at[d - 1], rg.at[d - 1], ep_at(d), T)

    def forward(d):
        return send(rx.at[C, d], rx.at[C, d], sf.at[d], rf.at[d], E, pair)

    def forward_in(d):
        return send(rx.at[1 - C, d], rx.at[1 - C, d], sf.at[d], rf.at[d], E, pair)

    loop(1, 16, lambda d: dispatch(d).start())
    forward(0).start()

    to_pair(rm.at[1 - C], rm.at[1 - C], 1).wait_recv()
    ms = jnp.zeros((32, 1), F32)
    for t in range(16):
        v = rm[t % 2, t // 2].astype(F32)
        ms = ms + jnp.sum(v * v, axis=1, keepdims=True)
    scale = lax.rsqrt(ms * (1.0 / 2048) + EPS)
    logit = jnp.zeros((32, 128), F32)
    for t in range(16):
        v = rm[t % 2, t // 2].astype(F32)
        n = (v * scale * fgain[t : t + 1, :]).astype(BF16)
        xd[:, lanes(t)] = n
        logit = logit + n.astype(F32) * blend[t : t + 1, :].astype(F32)
    mix_weight = jax.nn.sigmoid(jnp.sum(logit, axis=1, keepdims=True))
    hid = dot(xd[...], dgu[...])
    hid = (silu(hid[:, 0:128]) * hid[:, 128:256]).astype(BF16)
    part = dot(hid, ddn[...]) * mix_weight
    for t in range(16):
        half_d[t % 2, t // 2] = part[:, lanes(t)].astype(BF16)
        if t % 2 == 0:
            own_d[t // 2] = jnp.where(C == 0, part[:, lanes(t)], part[:, lanes(t + 1)])
    swap_dense = to_pair(half_d.at[1 - C], pair_d, 2)
    swap_dense.start()

    def arrive(d):
        dispatch(d).wait_recv()
        forward(d).start()

    loop(1, 16, arrive)
    loop(0, 16, lambda d: forward_in(d).wait_recv())

    def side(c):
        v = rx[c].astype(F32).reshape(16, 2, 8, 512)
        return v[:, 0].reshape(128, 512), v[:, 1].reshape(128, 512)

    quarters = [side(0), side(1)]
    ms = jnp.zeros((128, 1), F32)
    for q in quarters:
        for v in q:
            ms = ms + jnp.sum(v * v, axis=1, keepdims=True)
    scale = lax.rsqrt(ms * (1.0 / 2048) + EPS)
    for t in range(16):
        zz = t // 2
        v = quarters[t % 2][zz // 4][:, lanes(zz % 4)]
        xn[:, lanes(t)] = (v * scale * fgain[t : t + 1, :]).astype(BF16)
    row = lax.broadcasted_iota(jnp.int32, (128, 128), 0)
    hids = []
    for j in range(2):
        hid = dot(xn[...], gu[j])
        hid = silu(hid[:, 0:128]) * hid[:, 128:256]
        mine = (row % 8 >= 4) if j else (row % 8 < 4)
        hids.append(jnp.where(mine, hid, 0.0).astype(BF16))
    part = dot(jnp.concatenate(hids, axis=1), dn[...].reshape(256, 2048))

    def folded(v):
        lo = v[0].reshape(16, 8, 512)
        hi = v[1].reshape(16, 8, 512)
        return jnp.concatenate([lo, hi], axis=1)

    for q in range(2):
        even = jnp.concatenate([part[:, lanes(2 * z)] for z in range(4 * q, 4 * q + 4)], axis=1)
        odd = jnp.concatenate([part[:, lanes(2 * z + 1)] for z in range(4 * q, 4 * q + 4)], axis=1)
        half_e[0, q] = even.astype(BF16)
        half_e[1, q] = odd.astype(BF16)
        own_e[q] = jnp.where(C == 0, even, odd)
    swap_expert = to_pair(half_e.at[1 - C], pair_e, 3)
    swap_expert.start()
    swap_expert.wait_recv()
    both = own_e[...] + pair_e[...].astype(F32)
    ret[...] = folded(both).astype(BF16)
    back[E] = ret[0]

    def give_back(d):
        return send(ret.at[d], back.at[E], sr.at[d - 1], rr.at[d - 1], ep_from(d), T)

    def give_back_in(d):
        return send(ret.at[d], back.at[ep_at(d)], sr.at[d - 1], rr.at[d - 1], ep_from(d), T)

    loop(1, 16, lambda d: give_back(d).start())
    swap_dense.wait_recv()
    own_d[...] = own_d[...] + pair_d[...].astype(F32)
    weight = place[1]
    w_hi = weight.astype(BF16)
    w_lo = (weight - w_hi.astype(F32)).astype(BF16)
    loop(1, 16, lambda d: give_back_in(d).wait_recv())
    v = back[...].astype(F32).reshape(16, 2, 8, 512)
    first = (((0,), (0,)), ((), ()))
    for q in range(2):
        rows = v[:, q].reshape(128, 512).astype(BF16)
        mix = dot(w_hi, rows, first) + dot(w_lo, rows, first)
        for z in range(4):
            own_d[4 * q + z] = own_d[4 * q + z] + mix[:, lanes(z)]
    rs2_out[...] = own_d[...].astype(BF16)

    def scatter2(d):
        return send(
            rs2_out.at[z_block(d)], rs2_in.at[d - 1], sz.at[d + 13], rz.at[d + 13], E, tp_at(d)
        )

    loop(1, 8, lambda d: scatter2(d).start())
    total = own_d[Z] + rm[C, Z].astype(F32)
    loop(1, 8, lambda d: scatter2(d).wait_recv())
    for d in range(7):
        total = total + rs2_in[d].astype(F32)
    lout[...] = total.astype(BF16)
    done = pltpu.make_async_copy(lout, layer_out, store_sem.at[2])
    done.start()

    for f in (w_p, w_q, n_p, n_q, back_p, back_q):
        loop(1, 4, lambda d, f=f: f(d).wait_send())
    for f in (scatter, gather, scatter2):
        loop(1, 8, lambda d, f=f: f(d).wait_send())
    for f in (dispatch, give_back):
        loop(1, 16, lambda d, f=f: f(d).wait_send())
    loop(0, 16, lambda d: forward(d).wait_send())
    for s in (swap_mixer, swap_resid, swap_dense, swap_expert):
        s.wait_send()
    keep_state.wait()
    keep_conv.wait()
    done.wait()


SCRATCH = [
    ((32, 2048), BF16),
    ((16, 128), F32),
    ((16, 128), F32),
    ((16, 128), F32),
    ((16, 128), BF16),
    ((3, 4, 128), F32),
    ((32, 2048), BF16),
    ((2, 32), jnp.int32),
    ((2, 32), F32),
    ((3, 3, 32, 128), BF16),
    ((32, 2, 64, 128), F32),
    ((4, 128, 256), BF16),
    ((4, 128, 256), BF16),
    ((128, 2048), BF16),
    ((2, 2048, 256), BF16),
    ((2, 128, 2048), BF16),
    ((2048, 256), BF16),
    ((128, 2048), BF16),
    ((32, 2048), BF16),
    ((4, 32, 512), BF16),
    ((4, 32, 512), BF16),
    ((4, 32, 512), BF16),
    ((4, 32, 512), BF16),
    ((4, 32, 256), BF16),
    ((4, 32, 256), BF16),
    ((3, 32, 256), BF16),
    ((3, 32, 256), BF16),
    ((2, 32, 128), F32),
    ((32, 128), F32),
    ((32, 128), F32),
    ((32, 128), F32),
    ((32, 128), F32),
    ((3, 32, 128), BF16),
    ((2, 8, 32, 128), BF16),
    ((8, 32, 128), F32),
    ((8, 32, 128), BF16),
    ((8, 32, 128), BF16),
    ((7, 32, 128), BF16),
    ((2, 8, 32, 128), BF16),
    ((8, 128), F32),
    ((2, 128, 32), F32),
    ((16, 16, 512), BF16),
    ((2, 16, 16, 512), BF16),
    ((128, 2048), BF16),
    ((2, 2, 128, 512), BF16),
    ((2, 128, 512), F32),
    ((2, 128, 512), BF16),
    ((16, 16, 512), BF16),
    ((16, 16, 512), BF16),
    ((32, 2048), BF16),
    ((2, 8, 32, 128), BF16),
    ((8, 32, 128), F32),
    ((8, 32, 128), BF16),
    ((8, 32, 128), BF16),
    ((7, 32, 128), BF16),
    ((32, 128), BF16),
]


def on_device(*args):
    (
        residual,
        mixer_gain,
        gate_proj,
        input_proj,
        write_proj,
        read_proj,
        step_proj,
        conv_weight,
        step_bias,
        log_rate,
        skip_gain,
        group_gain,
        ssm_state,
        conv_state,
        out_proj,
        ffn_gain,
        routes,
        route_weight,
        expert_gate,
        expert_up,
        expert_down,
        dense_gate,
        dense_up,
        dense_down,
        blend_weight,
    ) = args
    conv_t = jnp.transpose(conv_state, (1, 2, 0, 3))
    layer_out, new_state, newest = pl.pallas_call(
        kernel,
        out_shape=(
            jax.ShapeDtypeStruct((32, 128), BF16),
            jax.ShapeDtypeStruct((32, 2, 64, 128), F32),
            jax.ShapeDtypeStruct((3, 32, 128), BF16),
        ),
        in_specs=[ANY] * 8 + [SMEM] * 3 + [ANY] * 14,
        out_specs=(ANY, ANY, ANY),
        scratch_shapes=[pltpu.VMEM(s, d) for s, d in SCRATCH]
        + [
            pltpu.SemaphoreType.DMA((24,)),
            pltpu.SemaphoreType.DMA((3,)),
            pltpu.SemaphoreType.DMA((12,)),
            pltpu.SemaphoreType.DMA((12,)),
            pltpu.SemaphoreType.DMA((6,)),
            pltpu.SemaphoreType.DMA((6,)),
            pltpu.SemaphoreType.DMA((21,)),
            pltpu.SemaphoreType.DMA((21,)),
            pltpu.SemaphoreType.DMA((4,)),
            pltpu.SemaphoreType.DMA((4,)),
            pltpu.SemaphoreType.DMA((15,)),
            pltpu.SemaphoreType.DMA((15,)),
            pltpu.SemaphoreType.DMA((16,)),
            pltpu.SemaphoreType.DMA((16,)),
            pltpu.SemaphoreType.DMA((15,)),
            pltpu.SemaphoreType.DMA((15,)),
        ],
        compiler_params=pltpu.CompilerParams(
            collective_id=0, has_side_effects=True, vmem_limit_bytes=67043328
        ),
    )(
        residual,
        mixer_gain.reshape(16, 128),
        gate_proj,
        input_proj,
        write_proj,
        read_proj,
        step_proj.T,
        jnp.transpose(conv_weight, (1, 0, 2)),
        step_bias,
        log_rate,
        skip_gain,
        group_gain.reshape(16, 128),
        ssm_state,
        conv_t,
        out_proj,
        ffn_gain.reshape(16, 128),
        routes.T,
        route_weight.T,
        expert_gate,
        expert_up,
        expert_down,
        dense_gate,
        dense_up,
        dense_down,
        blend_weight.reshape(16, 128),
    )
    new_conv = jnp.concatenate([conv_t[1:], newest[None]], axis=0)
    return layer_out, new_state, jnp.transpose(new_conv, (2, 0, 1, 3))


def solution(mesh):
    return jax.shard_map(
        on_device,
        mesh=mesh,
        in_specs=(
            P("ep", None),
            P(),
            P("ep", "tp"),
            P("ep", "tp"),
            P("ep", "tp"),
            P("ep", "tp"),
            P(),
            P(),
            P(),
            P(),
            P(),
            P(),
            P("ep", "tp", None, None),
            P("ep", None, None, "tp"),
            P("tp", None),
            P(),
            P("ep", None),
            P("ep", None),
            P("ep", None, "tp"),
            P("ep", None, "tp"),
            P("ep", "tp", None),
            P(None, "tp"),
            P(None, "tp"),
            P("tp", None),
            P(),
        ),
        out_specs=(P("ep", "tp"), P("ep", "tp", None, None), P("ep", None, None, "tp")),
        check_vma=False,
    )
```

```python
import functools

import jax
import jax.numpy as jnp
from jax import lax
from jax.experimental import pallas as pl
from jax.experimental.pallas import tpu as pltpu
from jax.sharding import PartitionSpec as P

MESH = pl.DeviceIdType.MESH
F32 = jnp.float32
BF16 = jnp.bfloat16
EPS = 1e-06
VM = pl.BlockSpec(memory_space=pltpu.VMEM)
ANY = pl.BlockSpec(memory_space=pl.ANY)
HBM = pl.BlockSpec(memory_space=pltpu.HBM)


def dot(a, b, dims=(((1,), (0,)), ((), ()))):
    return lax.dot_general(a, b, dims, preferred_element_type=F32)


def silu(v):
    return v * jax.nn.sigmoid(v)


def lanes(t):
    return slice(t * 128, (t + 1) * 128)


def kernel(
    residual,
    mixer_gain,
    gate_proj,
    input_proj,
    write_proj,
    read_proj,
    step_proj,
    conv_weight,
    step_bias,
    log_rate,
    skip_gain,
    group_gain,
    ssm_state,
    conv_state,
    out_proj,
    ffn_gain,
    routes,
    route_weight,
    expert_gate,
    expert_up,
    expert_down,
    dense_gate,
    dense_up,
    dense_down,
    blend_weight,
    layer_out,
    new_state,
    new_conv,
    res,
    mgain,
    ggain,
    fgain,
    blend,
    cw,
    heads,
    sproj,
    rts,
    rw,
    cst,
    st,
    st_hi,
    st_lo,
    wp,
    wq,
    op,
    gu,
    dn,
    dgu,
    ddn,
    nat,
    np_,
    nq,
    rp,
    rq,
    sp,
    sq,
    r2p,
    r2q,
    dec,
    dxs,
    bs,
    mixer_half,
    mixer_own,
    mixer_pair,
    rs_out,
    rs_in,
    rm,
    place,
    outb,
    rx,
    xn,
    half_e,
    own_e,
    pair_e,
    ret,
    back,
    xd,
    half_d,
    own_d,
    pair_d,
    rs2_out,
    rs2_in,
    load_sem,
    s1,
    r1,
    s2,
    r2,
    sz,
    rz,
    spair,
    rpair,
    sg,
    rg,
    sf,
    rf,
    sr,
    rr,
):
    E = lax.axis_index("ep")
    T = lax.axis_index("tp")
    Y, X = lax.div(E, 4), lax.rem(E, 4)
    Z, C = lax.div(T, 2), lax.rem(T, 2)
    pair = Z * 2 + (1 - C)

    def ep_at(d):
        dy, dx = lax.div(d, 4), lax.rem(d, 4)
        return lax.rem(Y + dy, 4) * 4 + lax.rem(X + dx, 4)

    def ep_from(d):
        dy, dx = lax.div(d, 4), lax.rem(d, 4)
        return lax.rem(Y + 4 - dy, 4) * 4 + lax.rem(X + 4 - dx, 4)

    def tp_at(d):
        return lax.rem(Z + d, 8) * 2 + C

    def loop(lo, hi, fn):
        lax.fori_loop(lo, hi, lambda i, c: (fn(i), c)[1], 0)

    def send(src, dst, ssem, rsem, ep, tp):
        return pltpu.make_async_remote_copy(
            src_ref=src,
            dst_ref=dst,
            send_sem=ssem,
            recv_sem=rsem,
            device_id={"ep": ep, "tp": tp},
            device_id_type=MESH,
        )

    bar = pltpu.get_barrier_semaphore()
    loop(
        1,
        16,
        lambda d: pl.semaphore_signal(
            bar, inc=1, device_id={"ep": ep_at(d), "tp": T}, device_id_type=MESH
        ),
    )
    loop(
        1,
        8,
        lambda d: pl.semaphore_signal(
            bar, inc=1, device_id={"ep": E, "tp": tp_at(d)}, device_id_type=MESH
        ),
    )
    pl.semaphore_signal(bar, inc=1, device_id={"ep": E, "tp": pair}, device_id_type=MESH)

    chan = pl.ds(pl.multiple_of(T * 128, 128), 128)
    loads = {}

    def load(name, *pairs):
        first = sum(len(v) for v in loads.values())
        copies = [
            pltpu.make_async_copy(s, d, load_sem.at[first + i]) for i, (s, d) in enumerate(pairs)
        ]
        for c in copies:
            c.start()
        loads[name] = copies

    def loaded(*names):
        for name in names:
            for c in loads[name]:
                c.wait()

    load("res", (residual, res), (mixer_gain, mgain))
    load(
        "proj",
        (gate_proj, wp.at[X, :, pl.ds(0, 128)]),
        (input_proj, wp.at[X, :, pl.ds(128, 128)]),
        (write_proj, wq.at[Y, :, pl.ds(0, 128)]),
        (read_proj, wq.at[Y, :, pl.ds(128, 128)]),
    )
    load(
        "small",
        (step_proj, sproj),
        (step_bias, heads.at[0]),
        (log_rate, heads.at[1]),
        (skip_gain, heads.at[2]),
        (conv_weight.at[:, :, chan], cw),
        (conv_state, cst),
        (routes, rts),
        (route_weight, rw),
    )
    load("state", (ssm_state, st))
    load("op", (out_proj, op), (group_gain, ggain))
    load("ffn", (ffn_gain, fgain), (blend_weight, blend))
    load(
        "dense",
        (dense_gate, dgu.at[:, pl.ds(0, 128)]),
        (dense_up, dgu.at[:, pl.ds(128, 128)]),
        (dense_down, ddn),
    )
    load(
        "experts",
        (expert_gate, gu.at[:, :, pl.ds(0, 128)]),
        (expert_up, gu.at[:, :, pl.ds(128, 128)]),
        (expert_down, dn),
    )

    loaded("res")
    rv = res[...].astype(F32)
    scale = lax.rsqrt(jnp.mean(rv * rv, axis=-1, keepdims=True) + EPS)
    for t in range(16):
        blk = (rv[:, lanes(t)] * scale * mgain[t : t + 1, :]).astype(BF16)
        nat[:, lanes(t)] = blk
        np_[t // 4, :, lanes(t % 4)] = blk
        nq[t % 4, :, lanes(t // 4)] = blk
    rp[0] = np_[Y]
    rq[0] = nq[X]

    loaded("proj")
    pl.semaphore_wait(bar, 23)

    def y_at(d):
        return lax.rem(Y + d, 4) * 4 + X

    def x_at(d):
        return Y * 4 + lax.rem(X + d, 4)

    def w_p(d):
        return send(wp.at[X], wp.at[X], s1.at[d - 1], r1.at[d - 1], x_at(d), T)

    def w_q(d):
        return send(wq.at[Y], wq.at[Y], s1.at[d + 2], r1.at[d + 2], y_at(d), T)

    def n_p(d):
        return send(
            np_.at[lax.rem(Y + d, 4)], rp.at[d], s1.at[d + 5], r1.at[d + 5], y_at(d), T
        )

    def n_q(d):
        return send(
            nq.at[lax.rem(X + d, 4)], rq.at[d], s1.at[d + 8], r1.at[d + 8], x_at(d), T
        )

    for f in (w_p, w_q, n_p, n_q):
        loop(1, 4, lambda d, f=f: f(d).start())

    loaded("small")
    raw = dot(nat[...], sproj[...], (((1,), (1,)), ((), ())))
    lane32 = lax.broadcasted_iota(jnp.int32, (32, 32), 1)
    lane128 = lax.broadcasted_iota(jnp.int32, (32, 128), 1)
    head_row = lane32[0:1]

    def of_head(i, h):
        return jnp.sum(jnp.where(head_row == 2 * T + h, heads[i], 0.0), axis=1, keepdims=True)

    dts, decays = [], []
    for h in range(2):
        col = jnp.sum(jnp.where(lane32 == 2 * T + h, raw, 0.0), axis=1, keepdims=True)
        v = jnp.broadcast_to(col, (32, 128)) + of_head(0, h)
        dt = jnp.maximum(v, 0.0) + jnp.log1p(jnp.exp(-jnp.abs(v)))
        rate = jnp.exp(jnp.broadcast_to(of_head(1, h), (32, 128)))
        decays.append(jnp.exp(-rate * dt))
        dec[h] = decays[h]
        dts.append(dt)
    dt = jnp.where(lane128 < 64, dts[0], dts[1])
    decay = jnp.where(lane128 < 64, decays[0], decays[1])
    skip = jnp.where(lane128 < 64, of_head(2, 0), of_head(2, 1))
    held = []
    for c in range(3):
        acc = cst[0, c].astype(F32) * cw[c, 0:1, :]
        for k in range(1, 3):
            acc = acc + cst[k, c].astype(F32) * cw[c, k : k + 1, :]
        held.append(acc)

    sub32 = lax.broadcasted_iota(jnp.int32, (32, 32), 0)
    hot = [(sub32 == rts[k : k + 1, :]).astype(F32) for k in range(2)]
    before = (sub32 < lane32).astype(BF16)
    prefix = dot((hot[0] + hot[1]).astype(BF16), before)
    slot = lax.broadcasted_iota(jnp.int32, (128, 32), 0)
    spots = []
    for k in range(2):
        rank = jnp.sum(hot[k] * prefix, axis=0, keepdims=True).astype(jnp.int32)
        spots.append((slot == rts[k : k + 1, :] * 4 + rank).astype(F32))
    place[0] = spots[0] + spots[1]
    place[1] = spots[0] * rw[0:1, :] + spots[1] * rw[1:2, :]

    loaded("state")

    def split(s):
        v = st[s].reshape(128, 128)
        hi = v.astype(BF16)
        st_hi[s] = hi
        st_lo[s] = (v - hi.astype(F32)).astype(BF16)

    loop(0, 32, split)
    for k in range(2):
        for c in range(3):
            new_conv[k, c] = cst[k + 1, c]

    loop(1, 4, lambda d: w_p(d).wait_recv())
    loop(1, 4, lambda d: n_p(d).wait_recv())
    part_p = dot(rp[...].reshape(128, 512), wp[...].reshape(512, 256))
    sp[...] = part_p.astype(BF16).reshape(4, 32, 256)

    def back_p(d):
        return send(
            sp.at[d], r2p.at[d - 1], s2.at[d - 1], r2.at[d - 1], y_at(4 - d), T
        )

    loop(1, 4, lambda d: back_p(d).start())
    loop(1, 4, lambda d: w_q(d).wait_recv())
    loop(1, 4, lambda d: n_q(d).wait_recv())
    part_q = dot(rq[...].reshape(128, 512), wq[...].reshape(512, 256))
    sq[...] = part_q.astype(BF16).reshape(4, 32, 256)

    def back_q(d):
        return send(
            sq.at[d], r2q.at[d - 1], s2.at[d + 2], r2.at[d + 2], x_at(4 - d), T
        )

    loop(1, 4, lambda d: back_q(d).start())
    own_p, own_q = part_p[0:32], part_q[0:32]
    loaded("op")
    loop(1, 4, lambda d: back_p(d).wait_recv())
    for d in range(3):
        own_p = own_p + r2p[d].astype(F32)
    loop(1, 4, lambda d: back_q(d).wait_recv())
    for d in range(3):
        own_q = own_q + r2q[d].astype(F32)
    z_proj = own_p[:, 0:128].astype(BF16).astype(F32)
    fresh = [own_p[:, 128:256], own_q[:, 0:128], own_q[:, 128:256]]
    acts = []
    for c in range(3):
        row = fresh[c].astype(BF16)
        new_conv[2, c] = row
        acts.append(silu(held[c] + row.astype(F32) * cw[c, 3:4, :]))
    x_act = acts[0]

    write, read = acts[1], acts[2]
    read_hi = read.astype(BF16)
    read_lo = (read - read_hi.astype(F32)).astype(BF16)
    last = (((1,), (1,)), ((), ()))
    sub8 = lax.broadcasted_iota(jnp.int32, (8, 128), 0)
    outs = []
    for g in range(4):
        eight = slice(8 * g, 8 * g + 8)
        hi = st_hi[eight].reshape(1024, 128)
        lo = st_lo[eight].reshape(1024, 128)
        two = jnp.concatenate([read_hi[eight], read_lo[eight]], axis=0)
        r = dot(two, hi, last)
        r = r[0:8] + r[8:16] + dot(read_hi[eight], lo, last)
        y = jnp.zeros((8, 128), F32)
        for i in range(8):
            y = jnp.where(sub8 == i, r[:, lanes(i)], y)
        outs.append(y)
    step_x = dt * x_act
    ssm_out = decay * jnp.concatenate(outs, axis=0) + step_x * jnp.sum(
        write * read, axis=1, keepdims=True
    )
    dxs[...] = step_x
    bs[...] = write

    def tokens(g):
        base = pl.multiple_of(g * 8, 8)
        dx_t = jnp.transpose(dxs[pl.ds(base, 8), :])
        for i in range(8):
            s = base + i
            b_row = bs[pl.ds(s, 1), :]
            for h in range(2):
                new_state[s, h] = (
                    dec[h, pl.ds(s, 1), :] * st[s, h]
                    + dx_t[h * 64 : h * 64 + 64, i : i + 1] * b_row
                )

    gated = (ssm_out + skip * x_act) * silu(z_proj)
    gated = gated * lax.rsqrt(jnp.mean(gated * gated, axis=-1, keepdims=True) + EPS)
    mixed = (gated * ggain[pl.ds(T, 1), :]).astype(BF16)
    part = dot(mixed, op[...])
    for t in range(16):
        mixer_half[t % 2, t // 2] = part[:, lanes(t)].astype(BF16)
        if t % 2 == 0:
            mixer_own[t // 2] = jnp.where(C == 0, part[:, lanes(t)], part[:, lanes(t + 1)])

    def to_pair(src, dst, i):
        return send(src, dst, spair.at[i], rpair.at[i], E, pair)

    swap_mixer = to_pair(mixer_half.at[1 - C], mixer_pair, 0)
    swap_mixer.start()
    swap_mixer.wait_recv()
    mixer_own[...] = mixer_own[...] + mixer_pair[...].astype(F32)
    rs_out[...] = mixer_own[...].astype(BF16)

    def z_block(d):
        return lax.rem(Z + d, 8)

    def scatter(d):
        return send(
            rs_out.at[z_block(d)], rs_in.at[d - 1], sz.at[d - 1], rz.at[d - 1], E, tp_at(d)
        )

    loop(1, 8, lambda d: scatter(d).start())
    total = mixer_own[Z]
    loop(0, 2, tokens)
    resid_cols = res[:, chan].astype(F32)
    loop(1, 8, lambda d: scatter(d).wait_recv())
    for d in range(7):
        total = total + rs_in[d].astype(F32)
    rm[C, Z] = (resid_cols + total).astype(BF16)

    def gather(d):
        return send(
            rm.at[C, Z], rm.at[C, Z], sz.at[d + 6], rz.at[d + 6], E, tp_at(d)
        )

    def gather_in(d):
        return send(
            rm.at[C, z_block(8 - d)], rm.at[C, z_block(8 - d)], sz.at[d + 6], rz.at[d + 6], E, tp_at(d)
        )

    loop(1, 8, lambda d: gather(d).start())
    loop(2, 4, tokens)
    loaded("dense", "experts", "ffn")
    loop(1, 8, lambda d: gather_in(d).wait_recv())
    swap_resid = to_pair(rm.at[C], rm.at[C], 1)
    swap_resid.start()

    mine = rm[C]
    mine = jnp.concatenate([mine[z] for z in range(8)], axis=1)
    rows = dot(place[0].astype(BF16), mine).reshape(16, 8, 1024)
    outb[...] = jnp.concatenate([rows[:, :, :512], rows[:, :, 512:]], axis=1).astype(BF16)
    rx[C, 0] = outb[E]

    def dispatch(d):
        return send(outb.at[ep_at(d)], rx.at[C, d], sg.at[d - 1], rg.at[d - 1], ep_at(d), T)

    def forward(d):
        return send(rx.at[C, d], rx.at[C, d], sf.at[d], rf.at[d], E, pair)

    def forward_in(d):
        return send(rx.at[1 - C, d], rx.at[1 - C, d], sf.at[d], rf.at[d], E, pair)

    loop(1, 16, lambda d: dispatch(d).start())
    forward(0).start()

    to_pair(rm.at[1 - C], rm.at[1 - C], 1).wait_recv()
    ms = jnp.zeros((32, 1), F32)
    for t in range(16):
        v = rm[t % 2, t // 2].astype(F32)
        ms = ms + jnp.sum(v * v, axis=1, keepdims=True)
    scale = lax.rsqrt(ms * (1.0 / 2048) + EPS)
    logit = jnp.zeros((32, 128), F32)
    for t in range(16):
        v = rm[t % 2, t // 2].astype(F32)
        n = (v * scale * fgain[t : t + 1, :]).astype(BF16)
        xd[:, lanes(t)] = n
        logit = logit + n.astype(F32) * blend[t : t + 1, :].astype(F32)
    mix_weight = jax.nn.sigmoid(jnp.sum(logit, axis=1, keepdims=True))
    hid = dot(xd[...], dgu[...])
    hid = (silu(hid[:, 0:128]) * hid[:, 128:256]).astype(BF16)
    part = dot(hid, ddn[...]) * mix_weight
    for t in range(16):
        half_d[t % 2, t // 2] = part[:, lanes(t)].astype(BF16)
        if t % 2 == 0:
            own_d[t // 2] = jnp.where(C == 0, part[:, lanes(t)], part[:, lanes(t + 1)])
    swap_dense = to_pair(half_d.at[1 - C], pair_d, 2)
    swap_dense.start()

    def arrive(d):
        dispatch(d).wait_recv()
        forward(d).start()

    loop(1, 16, arrive)
    loop(0, 16, lambda d: forward_in(d).wait_recv())

    def side(c):
        v = rx[c].astype(F32).reshape(16, 2, 8, 512)
        return v[:, 0].reshape(128, 512), v[:, 1].reshape(128, 512)

    quarters = [side(0), side(1)]
    ms = jnp.zeros((128, 1), F32)
    for q in quarters:
        for v in q:
            ms = ms + jnp.sum(v * v, axis=1, keepdims=True)
    scale = lax.rsqrt(ms * (1.0 / 2048) + EPS)
    for t in range(16):
        zz = t // 2
        v = quarters[t % 2][zz // 4][:, lanes(zz % 4)]
        xn[:, lanes(t)] = (v * scale * fgain[t : t + 1, :]).astype(BF16)
    row = lax.broadcasted_iota(jnp.int32, (128, 128), 0)
    hids = []
    for j in range(2):
        hid = dot(xn[...], gu[j])
        hid = silu(hid[:, 0:128]) * hid[:, 128:256]
        mine = (row % 8 >= 4) if j else (row % 8 < 4)
        hids.append(jnp.where(mine, hid, 0.0).astype(BF16))
    part = dot(jnp.concatenate(hids, axis=1), dn[...].reshape(256, 2048))

    def folded(v):
        lo = v[0].reshape(16, 8, 512)
        hi = v[1].reshape(16, 8, 512)
        return jnp.concatenate([lo, hi], axis=1)

    for q in range(2):
        even = jnp.concatenate([part[:, lanes(2 * z)] for z in range(4 * q, 4 * q + 4)], axis=1)
        odd = jnp.concatenate([part[:, lanes(2 * z + 1)] for z in range(4 * q, 4 * q + 4)], axis=1)
        half_e[0, q] = even.astype(BF16)
        half_e[1, q] = odd.astype(BF16)
        own_e[q] = jnp.where(C == 0, even, odd)
    swap_expert = to_pair(half_e.at[1 - C], pair_e, 3)
    swap_expert.start()
    swap_expert.wait_recv()
    both = own_e[...] + pair_e[...].astype(F32)
    ret[...] = folded(both).astype(BF16)
    back[E] = ret[0]

    def give_back(d):
        return send(ret.at[d], back.at[E], sr.at[d - 1], rr.at[d - 1], ep_from(d), T)

    def give_back_in(d):
        return send(ret.at[d], back.at[ep_at(d)], sr.at[d - 1], rr.at[d - 1], ep_from(d), T)

    loop(1, 16, lambda d: give_back(d).start())
    swap_dense.wait_recv()
    own_d[...] = own_d[...] + pair_d[...].astype(F32)
    weight = place[1]
    w_hi = weight.astype(BF16)
    w_lo = (weight - w_hi.astype(F32)).astype(BF16)
    loop(1, 16, lambda d: give_back_in(d).wait_recv())
    v = back[...].astype(F32).reshape(16, 2, 8, 512)
    first = (((0,), (0,)), ((), ()))
    for q in range(2):
        rows = v[:, q].reshape(128, 512).astype(BF16)
        mix = dot(w_hi, rows, first) + dot(w_lo, rows, first)
        for z in range(4):
            own_d[4 * q + z] = own_d[4 * q + z] + mix[:, lanes(z)]
    rs2_out[...] = own_d[...].astype(BF16)

    def scatter2(d):
        return send(
            rs2_out.at[z_block(d)], rs2_in.at[d - 1], sz.at[d + 13], rz.at[d + 13], E, tp_at(d)
        )

    loop(1, 8, lambda d: scatter2(d).start())
    total = own_d[Z] + rm[C, Z].astype(F32)
    loop(1, 8, lambda d: scatter2(d).wait_recv())
    for d in range(7):
        total = total + rs2_in[d].astype(F32)
    layer_out[...] = total.astype(BF16)

    for f in (w_p, w_q, n_p, n_q, back_p, back_q):
        loop(1, 4, lambda d, f=f: f(d).wait_send())
    for f in (scatter, gather, scatter2):
        loop(1, 8, lambda d, f=f: f(d).wait_send())
    for f in (dispatch, give_back):
        loop(1, 16, lambda d, f=f: f(d).wait_send())
    loop(0, 16, lambda d: forward(d).wait_send())
    for s in (swap_mixer, swap_resid, swap_dense, swap_expert):
        s.wait_send()


def write_out(a, b, c, a_out, b_out, c_out, sem):
    copies = [
        pltpu.make_async_copy(src, dst, sem.at[i])
        for i, (src, dst) in enumerate(((b, b_out), (c, c_out), (a, a_out)))
    ]
    for copy in copies:
        copy.start()
    for copy in copies:
        copy.wait()


SCRATCH = [
    ((32, 2048), BF16),
    ((16, 128), F32),
    ((16, 128), F32),
    ((16, 128), F32),
    ((16, 128), BF16),
    ((3, 4, 128), F32),
    ((3, 1, 32), F32),
    ((32, 2048), BF16),
    ((2, 32), jnp.int32),
    ((2, 32), F32),
    ((3, 3, 32, 128), BF16),
    ((32, 2, 64, 128), F32),
    ((32, 128, 128), BF16),
    ((32, 128, 128), BF16),
    ((4, 128, 256), BF16),
    ((4, 128, 256), BF16),
    ((128, 2048), BF16),
    ((2, 2048, 256), BF16),
    ((2, 128, 2048), BF16),
    ((2048, 256), BF16),
    ((128, 2048), BF16),
    ((32, 2048), BF16),
    ((4, 32, 512), BF16),
    ((4, 32, 512), BF16),
    ((4, 32, 512), BF16),
    ((4, 32, 512), BF16),
    ((4, 32, 256), BF16),
    ((4, 32, 256), BF16),
    ((3, 32, 256), BF16),
    ((3, 32, 256), BF16),
    ((2, 32, 128), F32),
    ((32, 128), F32),
    ((32, 128), F32),
    ((2, 8, 32, 128), BF16),
    ((8, 32, 128), F32),
    ((8, 32, 128), BF16),
    ((8, 32, 128), BF16),
    ((7, 32, 128), BF16),
    ((2, 8, 32, 128), BF16),
    ((2, 128, 32), F32),
    ((16, 16, 512), BF16),
    ((2, 16, 16, 512), BF16),
    ((128, 2048), BF16),
    ((2, 2, 128, 512), BF16),
    ((2, 128, 512), F32),
    ((2, 128, 512), BF16),
    ((16, 16, 512), BF16),
    ((16, 16, 512), BF16),
    ((32, 2048), BF16),
    ((2, 8, 32, 128), BF16),
    ((8, 32, 128), F32),
    ((8, 32, 128), BF16),
    ((8, 32, 128), BF16),
    ((7, 32, 128), BF16),
]


def on_device(*args):
    (
        residual,
        mixer_gain,
        gate_proj,
        input_proj,
        write_proj,
        read_proj,
        step_proj,
        conv_weight,
        step_bias,
        log_rate,
        skip_gain,
        group_gain,
        ssm_state,
        conv_state,
        out_proj,
        ffn_gain,
        routes,
        route_weight,
        expert_gate,
        expert_up,
        expert_down,
        dense_gate,
        dense_up,
        dense_down,
        blend_weight,
    ) = args
    conv_t = jnp.transpose(conv_state, (1, 2, 0, 3))
    results = pl.pallas_call(
        kernel,
        out_shape=(
            pltpu.VMEM((32, 128), BF16),
            pltpu.VMEM((32, 2, 64, 128), F32),
            pltpu.VMEM((3, 3, 32, 128), BF16),
        ),
        in_specs=[HBM] * 25,
        out_specs=(VM, VM, VM),
        scratch_shapes=[pltpu.VMEM(s, d) for s, d in SCRATCH]
        + [
            pltpu.SemaphoreType.DMA((25,)),
            pltpu.SemaphoreType.DMA((12,)),
            pltpu.SemaphoreType.DMA((12,)),
            pltpu.SemaphoreType.DMA((6,)),
            pltpu.SemaphoreType.DMA((6,)),
            pltpu.SemaphoreType.DMA((21,)),
            pltpu.SemaphoreType.DMA((21,)),
            pltpu.SemaphoreType.DMA((4,)),
            pltpu.SemaphoreType.DMA((4,)),
            pltpu.SemaphoreType.DMA((15,)),
            pltpu.SemaphoreType.DMA((15,)),
            pltpu.SemaphoreType.DMA((16,)),
            pltpu.SemaphoreType.DMA((16,)),
            pltpu.SemaphoreType.DMA((15,)),
            pltpu.SemaphoreType.DMA((15,)),
        ],
        compiler_params=pltpu.CompilerParams(
            collective_id=0, has_side_effects=True, vmem_limit_bytes=64_400_000
        ),
    )(
        residual,
        mixer_gain.reshape(16, 128),
        gate_proj,
        input_proj,
        write_proj,
        read_proj,
        step_proj.T,
        jnp.transpose(conv_weight, (1, 0, 2)),
        step_bias.reshape(1, 32),
        log_rate.reshape(1, 32),
        skip_gain.reshape(1, 32),
        group_gain.reshape(16, 128),
        ssm_state,
        conv_t,
        out_proj,
        ffn_gain.reshape(16, 128),
        routes.T,
        route_weight.T,
        expert_gate,
        expert_up,
        expert_down,
        dense_gate,
        dense_up,
        dense_down,
        blend_weight.reshape(16, 128),
    )
    layer_out, new_state, new_conv = pl.pallas_call(
        write_out,
        out_shape=tuple(jax.ShapeDtypeStruct(r.shape, r.dtype) for r in results),
        in_specs=[ANY] * 3,
        out_specs=(HBM,) * 3,
        scratch_shapes=[pltpu.SemaphoreType.DMA((3,))],
        compiler_params=pltpu.CompilerParams(vmem_limit_bytes=1 << 20),
    )(*results)
    return layer_out, new_state, jnp.transpose(new_conv, (2, 0, 1, 3))


def solution(mesh):
    return jax.shard_map(
        on_device,
        mesh=mesh,
        in_specs=(
            P("ep", None),
            P(),
            P("ep", "tp"),
            P("ep", "tp"),
            P("ep", "tp"),
            P("ep", "tp"),
            P(),
            P(),
            P(),
            P(),
            P(),
            P(),
            P("ep", "tp", None, None),
            P("ep", None, None, "tp"),
            P("tp", None),
            P(),
            P("ep", None),
            P("ep", None),
            P("ep", None, "tp"),
            P("ep", None, "tp"),
            P("ep", "tp", None),
            P(None, "tp"),
            P(None, "tp"),
            P("tp", None),
            P(),
        ),
        out_specs=(P("ep", "tp"), P("ep", "tp", None, None), P("ep", None, None, "tp")),
        check_vma=False,
    )
```

```python
import functools

import jax
import jax.numpy as jnp
from jax import lax
from jax.experimental import pallas as pl
from jax.experimental.pallas import tpu as pltpu
from jax.sharding import PartitionSpec as P

MESH = pl.DeviceIdType.MESH
F32 = jnp.float32
BF16 = jnp.bfloat16
EPS = 1e-06
VM = pl.BlockSpec(memory_space=pltpu.VMEM)
ANY = pl.BlockSpec(memory_space=pl.ANY)
HBM = pl.BlockSpec(memory_space=pltpu.HBM)


def hops(d):
    dy, dx = divmod(d, 4)
    return min(dy, 4 - dy) + min(dx, 4 - dx)


FAR = sorted(range(1, 16), key=lambda d: -hops(d))
NEAR = FAR[::-1]
FAR_Z = (4, 3, 5, 2, 6, 1, 7)
NEAR_Z = FAR_Z[::-1]
FAR_LINE = (2, 1, 3)


def dot(a, b, dims=(((1,), (0,)), ((), ()))):
    return lax.dot_general(a, b, dims, preferred_element_type=F32)


def silu(v):
    return v * jax.nn.sigmoid(v)


def lanes(t):
    return slice(t * 128, (t + 1) * 128)


def kernel(
    residual,
    mixer_gain,
    gate_proj,
    input_proj,
    write_proj,
    read_proj,
    step_proj,
    conv_weight,
    step_bias,
    log_rate,
    skip_gain,
    group_gain,
    ssm_state,
    conv_state,
    out_proj,
    ffn_gain,
    routes,
    route_weight,
    expert_gate,
    expert_up,
    expert_down,
    dense_gate,
    dense_up,
    dense_down,
    blend_weight,
    layer_out,
    new_state,
    new_conv,
    res,
    mgain,
    ggain,
    fgain,
    blend,
    cw,
    heads,
    sproj,
    rts,
    rw,
    cst,
    st,
    st_hi,
    st_lo,
    wp,
    wq,
    op,
    gu,
    dn,
    dgu,
    ddn,
    nat,
    np_,
    nq,
    rp,
    rq,
    sp,
    sq,
    r2p,
    r2q,
    dec,
    dxs,
    bs,
    mixer_half,
    mixer_own,
    mixer_pair,
    rs_out,
    rs_in,
    rm,
    place,
    outb,
    rx,
    xn,
    half_e,
    own_e,
    pair_e,
    ret,
    back,
    xd,
    half_d,
    own_d,
    pair_d,
    rs2_out,
    rs2_in,
    load_sem,
    s1,
    r1,
    s2,
    r2,
    sz,
    rz,
    spair,
    rpair,
    sg,
    rg,
    sf,
    rf,
    sr,
    rr,
    sn,
    rn,
    near_sem,
    far_sem,
):
    E = lax.axis_index("ep")
    T = lax.axis_index("tp")
    Y, X = lax.div(E, 4), lax.rem(E, 4)
    Z, C = lax.div(T, 2), lax.rem(T, 2)
    pair = Z * 2 + (1 - C)

    def ep_at(d):
        dy, dx = divmod(d, 4)
        return lax.rem(Y + dy, 4) * 4 + lax.rem(X + dx, 4)

    def ep_from(d):
        dy, dx = divmod(d, 4)
        return lax.rem(Y + 4 - dy, 4) * 4 + lax.rem(X + 4 - dx, 4)

    def y_at(d):
        return lax.rem(Y + d, 4) * 4 + X

    def x_at(d):
        return Y * 4 + lax.rem(X + d, 4)

    def tp_at(d):
        return lax.rem(Z + d, 8) * 2 + C

    def loop(lo, hi, fn):
        lax.fori_loop(lo, hi, lambda i, c: (fn(i), c)[1], 0)

    def each(order, fn):
        for d in order:
            fn(d)

    def send(src, dst, ssem, rsem, ep, tp):
        return pltpu.make_async_remote_copy(
            src_ref=src,
            dst_ref=dst,
            send_sem=ssem,
            recv_sem=rsem,
            device_id={"ep": ep, "tp": tp},
            device_id_type=MESH,
        )

    chan = pl.ds(pl.multiple_of(T * 128, 128), 128)
    loads = {}

    def load(name, *pairs):
        first = sum(len(v) for v in loads.values())
        copies = [
            pltpu.make_async_copy(s, d, load_sem.at[first + i]) for i, (s, d) in enumerate(pairs)
        ]
        for c in copies:
            c.start()
        loads[name] = copies

    def loaded(*names):
        for name in names:
            for c in loads[name]:
                c.wait()

    load("res", (residual, res), (mixer_gain, mgain))
    load(
        "proj",
        (gate_proj, wp.at[X, :, pl.ds(0, 128)]),
        (input_proj, wp.at[X, :, pl.ds(128, 128)]),
        (write_proj, wq.at[Y, :, pl.ds(0, 128)]),
        (read_proj, wq.at[Y, :, pl.ds(128, 128)]),
    )
    def signal(sem, ep, tp):
        pl.semaphore_signal(
            sem, inc=1, device_id={"ep": ep, "tp": tp}, device_id_type=MESH
        )

    bar = pltpu.get_barrier_semaphore()
    each(FAR_LINE, lambda d: signal(bar, x_at(d), T))
    each(FAR_LINE, lambda d: signal(bar, y_at(d), T))
    each((1, 7), lambda d: signal(bar, E, tp_at(d)))
    signal(bar, E, pair)

    load(
        "small",
        (step_proj, sproj),
        (step_bias, heads.at[0]),
        (log_rate, heads.at[1]),
        (skip_gain, heads.at[2]),
        (conv_weight.at[:, :, chan], cw),
        (conv_state, cst),
        (routes, rts),
        (route_weight, rw),
    )
    load("state", (ssm_state, st))
    load("op", (out_proj, op), (group_gain, ggain))
    load("ffn", (ffn_gain, fgain), (blend_weight, blend))
    load(
        "dense",
        (dense_gate, dgu.at[:, pl.ds(0, 128)]),
        (dense_up, dgu.at[:, pl.ds(128, 128)]),
        (dense_down, ddn),
    )
    load(
        "experts",
        (expert_gate, gu.at[:, :, pl.ds(0, 128)]),
        (expert_up, gu.at[:, :, pl.ds(128, 128)]),
        (expert_down, dn),
    )

    loaded("res")
    rv = res[...].astype(F32)
    scale = lax.rsqrt(jnp.mean(rv * rv, axis=-1, keepdims=True) + EPS)
    for t in range(16):
        blk = (rv[:, lanes(t)] * scale * mgain[t : t + 1, :]).astype(BF16)
        nat[:, lanes(t)] = blk
        np_[t // 4, t % 4 // 2, :, lanes(t % 2)] = blk
        nq[t % 4, t // 8, :, lanes(t // 4 % 2)] = blk
    for h in range(2):
        rp[h, 0] = np_[Y, h]
        rq[h, 0] = nq[X, h]

    loaded("proj")
    pl.semaphore_wait(bar, 9)
    each((1, 7), lambda d: signal(near_sem, E, tp_at(d)))

    def w_p(d):
        return send(wp.at[X], wp.at[X], s1.at[d - 1], r1.at[d - 1], x_at(d), T)

    def w_q(d):
        return send(wq.at[Y], wq.at[Y], s1.at[d + 2], r1.at[d + 2], y_at(d), T)

    def n_p(d):
        return send(
            np_.at[lax.rem(Y + d, 4), C], rp.at[C, d], s1.at[d + 5], r1.at[d + 5], y_at(d), T
        )

    def n_q(d):
        return send(
            nq.at[lax.rem(X + d, 4), C], rq.at[C, d], s1.at[d + 8], r1.at[d + 8], x_at(d), T
        )

    for f in (n_p, n_q, w_p, w_q):
        each(FAR_LINE, lambda d, f=f: f(d).start())

    loaded("small")
    raw = dot(nat[...], sproj[...], (((1,), (1,)), ((), ())))
    lane32 = lax.broadcasted_iota(jnp.int32, (32, 32), 1)
    lane128 = lax.broadcasted_iota(jnp.int32, (32, 128), 1)
    head_row = lane32[0:1]

    def of_head(i, h):
        return jnp.sum(jnp.where(head_row == 2 * T + h, heads[i], 0.0), axis=1, keepdims=True)

    dts, decays = [], []
    for h in range(2):
        col = jnp.sum(jnp.where(lane32 == 2 * T + h, raw, 0.0), axis=1, keepdims=True)
        v = jnp.broadcast_to(col, (32, 128)) + of_head(0, h)
        dt = jnp.maximum(v, 0.0) + jnp.log1p(jnp.exp(-jnp.abs(v)))
        rate = jnp.exp(jnp.broadcast_to(of_head(1, h), (32, 128)))
        decays.append(jnp.exp(-rate * dt))
        dec[h] = decays[h]
        dts.append(dt)
    dt = jnp.where(lane128 < 64, dts[0], dts[1])
    decay = jnp.where(lane128 < 64, decays[0], decays[1])
    skip = jnp.where(lane128 < 64, of_head(2, 0), of_head(2, 1))
    held = []
    for c in range(3):
        acc = cst[0, c].astype(F32) * cw[c, 0:1, :]
        for k in range(1, 3):
            acc = acc + cst[k, c].astype(F32) * cw[c, k : k + 1, :]
        held.append(acc)

    sub32 = lax.broadcasted_iota(jnp.int32, (32, 32), 0)
    hot = [(sub32 == rts[k : k + 1, :]).astype(F32) for k in range(2)]
    before = (sub32 < lane32).astype(BF16)
    prefix = dot((hot[0] + hot[1]).astype(BF16), before)
    slot = lax.broadcasted_iota(jnp.int32, (128, 32), 0)
    spots = []
    for k in range(2):
        rank = jnp.sum(hot[k] * prefix, axis=0, keepdims=True).astype(jnp.int32)
        spots.append((slot == rts[k : k + 1, :] * 4 + rank).astype(F32))
    place[0] = spots[0] + spots[1]
    place[1] = spots[0] * rw[0:1, :] + spots[1] * rw[1:2, :]

    loaded("state")
    pl.semaphore_wait(near_sem, 2)
    each((2, 6), lambda d: signal(far_sem, E, tp_at(d)))

    def split(s):
        v = st[s].reshape(128, 128)
        hi = v.astype(BF16)
        st_hi[s] = hi
        st_lo[s] = (v - hi.astype(F32)).astype(BF16)

    loop(0, 32, split)
    for k in range(2):
        for c in range(3):
            new_conv[k, c] = cst[k + 1, c]

    def pass_p(side):
        return send(
            rp.at[side, pl.ds(1, 3)], rp.at[side, pl.ds(1, 3)], sn.at[0], rn.at[0], E, pair
        )

    def pass_q(side):
        return send(
            rq.at[side, pl.ds(1, 3)], rq.at[side, pl.ds(1, 3)], sn.at[1], rn.at[1], E, pair
        )

    each((1, 3, 2), lambda d: n_p(d).wait_recv())
    pass_p(C).start()
    each((1, 3, 2), lambda d: n_q(d).wait_recv())
    pass_q(C).start()
    pass_p(1 - C).wait_recv()
    each((1, 3, 2), lambda d: w_p(d).wait_recv())

    def projected(rows, weights):
        return dot(rows[0].reshape(128, 256), weights[0:2].reshape(256, 256)) + dot(
            rows[1].reshape(128, 256), weights[2:4].reshape(256, 256)
        )

    part_p = projected(rp, wp)
    sp[...] = part_p.astype(BF16).reshape(4, 32, 256)

    def back_p(d):
        return send(
            sp.at[d], r2p.at[d - 1], s2.at[d - 1], r2.at[d - 1], y_at(4 - d), T
        )

    each(FAR_LINE, lambda d: back_p(d).start())
    pass_q(1 - C).wait_recv()
    each((1, 3, 2), lambda d: w_q(d).wait_recv())
    part_q = projected(rq, wq)
    sq[...] = part_q.astype(BF16).reshape(4, 32, 256)

    def back_q(d):
        return send(
            sq.at[d], r2q.at[d - 1], s2.at[d + 2], r2.at[d + 2], x_at(4 - d), T
        )

    each(FAR_LINE, lambda d: back_q(d).start())
    pl.semaphore_wait(far_sem, 2)
    own_p, own_q = part_p[0:32], part_q[0:32]
    loaded("op")
    each((1, 3, 2), lambda d: back_p(d).wait_recv())
    for d in range(3):
        own_p = own_p + r2p[d].astype(F32)
    each((1, 3, 2), lambda d: back_q(d).wait_recv())
    for d in range(3):
        own_q = own_q + r2q[d].astype(F32)
    z_proj = own_p[:, 0:128].astype(BF16).astype(F32)
    fresh = [own_p[:, 128:256], own_q[:, 0:128], own_q[:, 128:256]]
    acts = []
    for c in range(3):
        row = fresh[c].astype(BF16)
        new_conv[2, c] = row
        acts.append(silu(held[c] + row.astype(F32) * cw[c, 3:4, :]))
    x_act = acts[0]

    write, read = acts[1], acts[2]
    read_hi = read.astype(BF16)
    read_lo = (read - read_hi.astype(F32)).astype(BF16)
    last = (((1,), (1,)), ((), ()))
    sub8 = lax.broadcasted_iota(jnp.int32, (8, 128), 0)
    outs = []
    for g in range(4):
        eight = slice(8 * g, 8 * g + 8)
        hi = st_hi[eight].reshape(1024, 128)
        lo = st_lo[eight].reshape(1024, 128)
        two = jnp.concatenate([read_hi[eight], read_lo[eight]], axis=0)
        r = dot(two, hi, last)
        r = r[0:8] + r[8:16] + dot(read_hi[eight], lo, last)
        y = jnp.zeros((8, 128), F32)
        for i in range(8):
            y = jnp.where(sub8 == i, r[:, lanes(i)], y)
        outs.append(y)
    step_x = dt * x_act
    ssm_out = decay * jnp.concatenate(outs, axis=0) + step_x * jnp.sum(
        write * read, axis=1, keepdims=True
    )
    dxs[...] = step_x
    bs[...] = write

    def tokens(g):
        base = pl.multiple_of(g * 8, 8)
        dx_t = jnp.transpose(dxs[pl.ds(base, 8), :])
        for i in range(8):
            s = base + i
            b_row = bs[pl.ds(s, 1), :]
            for h in range(2):
                new_state[s, h] = (
                    dec[h, pl.ds(s, 1), :] * st[s, h]
                    + dx_t[h * 64 : h * 64 + 64, i : i + 1] * b_row
                )

    gated = (ssm_out + skip * x_act) * silu(z_proj)
    gated = gated * lax.rsqrt(jnp.mean(gated * gated, axis=-1, keepdims=True) + EPS)
    mixed = (gated * ggain[pl.ds(T, 1), :]).astype(BF16)
    part = dot(mixed, op[...])
    for t in range(16):
        mixer_half[t % 2, t // 2] = part[:, lanes(t)].astype(BF16)
        if t % 2 == 0:
            mixer_own[t // 2] = jnp.where(C == 0, part[:, lanes(t)], part[:, lanes(t + 1)])

    def to_pair(src, dst, i):
        return send(src, dst, spair.at[i], rpair.at[i], E, pair)

    swap_mixer = to_pair(mixer_half.at[1 - C], mixer_pair, 0)
    swap_mixer.start()
    swap_mixer.wait_recv()
    mixer_own[...] = mixer_own[...] + mixer_pair[...].astype(F32)
    rs_out[...] = mixer_own[...].astype(BF16)

    def z_block(d):
        return lax.rem(Z + d, 8)

    def scatter(d):
        return send(
            rs_out.at[z_block(d)], rs_in.at[d - 1], sz.at[d - 1], rz.at[d - 1], E, tp_at(d)
        )

    each(FAR_Z, lambda d: scatter(d).start())
    total = mixer_own[Z]
    loop(0, 2, tokens)
    resid_cols = res[:, chan].astype(F32)
    each(NEAR_Z, lambda d: scatter(d).wait_recv())
    for d in range(7):
        total = total + rs_in[d].astype(F32)
    rm[C, Z] = (resid_cols + total).astype(BF16)

    def gather(d):
        return send(
            rm.at[C, Z], rm.at[C, Z], sz.at[d + 6], rz.at[d + 6], E, tp_at(d)
        )

    def gather_in(d):
        return send(
            rm.at[C, z_block(8 - d)], rm.at[C, z_block(8 - d)], sz.at[d + 6], rz.at[d + 6], E, tp_at(d)
        )

    each(FAR_Z, lambda d: gather(d).start())
    loop(2, 4, tokens)
    loaded("dense", "experts", "ffn")
    each(NEAR_Z, lambda d: gather_in(d).wait_recv())
    swap_resid = to_pair(rm.at[C], rm.at[C], 1)
    swap_resid.start()

    mine = rm[C]
    mine = jnp.concatenate([mine[z] for z in range(8)], axis=1)
    rows = dot(place[0].astype(BF16), mine).reshape(16, 8, 1024)
    outb[...] = jnp.concatenate([rows[:, :, :512], rows[:, :, 512:]], axis=1).astype(BF16)
    rx[C, 0] = outb[E]

    def dispatch(d):
        return send(outb.at[ep_at(d)], rx.at[C, d], sg.at[d - 1], rg.at[d - 1], ep_at(d), T)

    def forward(d):
        return send(rx.at[C, d], rx.at[C, d], sf.at[d], rf.at[d], E, pair)

    def forward_in(d):
        return send(rx.at[1 - C, d], rx.at[1 - C, d], sf.at[d], rf.at[d], E, pair)

    each(FAR, lambda d: dispatch(d).start())
    forward(0).start()

    to_pair(rm.at[1 - C], rm.at[1 - C], 1).wait_recv()
    ms = jnp.zeros((32, 1), F32)
    for t in range(16):
        v = rm[t % 2, t // 2].astype(F32)
        ms = ms + jnp.sum(v * v, axis=1, keepdims=True)
    scale = lax.rsqrt(ms * (1.0 / 2048) + EPS)
    logit = jnp.zeros((32, 128), F32)
    for t in range(16):
        v = rm[t % 2, t // 2].astype(F32)
        n = (v * scale * fgain[t : t + 1, :]).astype(BF16)
        xd[:, lanes(t)] = n
        logit = logit + n.astype(F32) * blend[t : t + 1, :].astype(F32)
    mix_weight = jax.nn.sigmoid(jnp.sum(logit, axis=1, keepdims=True))
    hid = dot(xd[...], dgu[...])
    hid = (silu(hid[:, 0:128]) * hid[:, 128:256]).astype(BF16)
    part = dot(hid, ddn[...]) * mix_weight
    for t in range(16):
        half_d[t % 2, t // 2] = part[:, lanes(t)].astype(BF16)
        if t % 2 == 0:
            own_d[t // 2] = jnp.where(C == 0, part[:, lanes(t)], part[:, lanes(t + 1)])
    swap_dense = to_pair(half_d.at[1 - C], pair_d, 2)
    swap_dense.start()

    def arrive(d):
        dispatch(d).wait_recv()
        forward(d).start()

    each(NEAR, arrive)
    each([0] + NEAR, lambda d: forward_in(d).wait_recv())

    def side(c):
        v = rx[c].astype(F32).reshape(16, 2, 8, 512)
        return v[:, 0].reshape(128, 512), v[:, 1].reshape(128, 512)

    quarters = [side(0), side(1)]
    ms = jnp.zeros((128, 1), F32)
    for q in quarters:
        for v in q:
            ms = ms + jnp.sum(v * v, axis=1, keepdims=True)
    scale = lax.rsqrt(ms * (1.0 / 2048) + EPS)
    for t in range(16):
        zz = t // 2
        v = quarters[t % 2][zz // 4][:, lanes(zz % 4)]
        xn[:, lanes(t)] = (v * scale * fgain[t : t + 1, :]).astype(BF16)
    row = lax.broadcasted_iota(jnp.int32, (128, 128), 0)
    hids = []
    for j in range(2):
        hid = dot(xn[...], gu[j])
        hid = silu(hid[:, 0:128]) * hid[:, 128:256]
        mine = (row % 8 >= 4) if j else (row % 8 < 4)
        hids.append(jnp.where(mine, hid, 0.0).astype(BF16))
    hid = jnp.concatenate(hids, axis=1)

    def swap_expert(q):
        return to_pair(half_e.at[1 - C, q], pair_e.at[q], 3 + q)

    for q in range(2):
        part = dot(hid, dn[:, :, q * 1024 : (q + 1) * 1024].reshape(256, 1024))
        even = jnp.concatenate([part[:, lanes(2 * z)] for z in range(4)], axis=1)
        odd = jnp.concatenate([part[:, lanes(2 * z + 1)] for z in range(4)], axis=1)
        half_e[0, q] = even.astype(BF16)
        half_e[1, q] = odd.astype(BF16)
        own_e[q] = jnp.where(C == 0, even, odd)
        swap_expert(q).start()

    def give_back(d, q):
        i = q * 15 + d - 1
        return send(ret.at[q, d], back.at[q, E], sr.at[i], rr.at[i], ep_from(d), T)

    def give_back_in(d, q):
        i = q * 15 + d - 1
        return send(ret.at[q, d], back.at[q, ep_at(d)], sr.at[i], rr.at[i], ep_from(d), T)

    for q in range(2):
        swap_expert(q).wait_recv()
        both = own_e[q] + pair_e[q].astype(F32)
        lo, hi = both[:, :256].reshape(16, 8, 256), both[:, 256:].reshape(16, 8, 256)
        ret[q] = jnp.concatenate([lo, hi], axis=1).astype(BF16)
        back[q, E] = ret[q, 0]
        each(FAR, lambda d, q=q: give_back(d, q).start())

    swap_dense.wait_recv()
    own_d[...] = own_d[...] + pair_d[...].astype(F32)
    weight = place[1]
    w_hi = weight.astype(BF16)
    w_lo = (weight - w_hi.astype(F32)).astype(BF16)
    for f in (w_p, w_q, n_p, n_q, back_p, back_q):
        loop(1, 4, lambda d, f=f: f(d).wait_send())
    for f in (scatter, gather):
        loop(1, 8, lambda d, f=f: f(d).wait_send())
    each(FAR, lambda d: dispatch(d).wait_send())
    loop(0, 16, lambda d: forward(d).wait_send())
    for c in (pass_p(C), pass_q(C), swap_mixer, swap_resid, swap_dense):
        c.wait_send()
    each(range(2), lambda q: swap_expert(q).wait_send())
    first = (((0,), (0,)), ((), ()))
    for q in range(2):
        each(NEAR, lambda d, q=q: give_back_in(d, q).wait_recv())
        v = back[q].astype(F32).reshape(16, 2, 8, 256)
        rows = jnp.concatenate([v[:, i].reshape(128, 256) for i in range(2)], axis=1)
        rows = rows.astype(BF16)
        mix = dot(w_hi, rows, first) + dot(w_lo, rows, first)
        for z in range(4):
            own_d[4 * q + z] = own_d[4 * q + z] + mix[:, lanes(z)]
    rs2_out[...] = own_d[...].astype(BF16)

    def scatter2(d):
        return send(
            rs2_out.at[z_block(d)], rs2_in.at[d - 1], sz.at[d + 13], rz.at[d + 13], E, tp_at(d)
        )

    each(FAR_Z, lambda d: scatter2(d).start())
    total = own_d[Z] + rm[C, Z].astype(F32)
    each(NEAR_Z, lambda d: scatter2(d).wait_recv())
    for d in range(7):
        total = total + rs2_in[d].astype(F32)
    layer_out[...] = total.astype(BF16)

    for q in range(2):
        each(FAR, lambda d, q=q: give_back(d, q).wait_send())
    loop(1, 8, lambda d: scatter2(d).wait_send())


def write_out(a, b, c, a_out, b_out, c_out, sem):
    copies = [
        pltpu.make_async_copy(src, dst, sem.at[i])
        for i, (src, dst) in enumerate(((b, b_out), (c, c_out), (a, a_out)))
    ]
    for copy in copies:
        copy.start()
    for copy in copies:
        copy.wait()


SCRATCH = [
    ((32, 2048), BF16),
    ((16, 128), F32),
    ((16, 128), F32),
    ((16, 128), F32),
    ((16, 128), BF16),
    ((3, 4, 128), F32),
    ((3, 1, 32), F32),
    ((32, 2048), BF16),
    ((2, 32), jnp.int32),
    ((2, 32), F32),
    ((3, 3, 32, 128), BF16),
    ((32, 2, 64, 128), F32),
    ((32, 128, 128), BF16),
    ((32, 128, 128), BF16),
    ((4, 128, 256), BF16),
    ((4, 128, 256), BF16),
    ((128, 2048), BF16),
    ((2, 2048, 256), BF16),
    ((2, 128, 2048), BF16),
    ((2048, 256), BF16),
    ((128, 2048), BF16),
    ((32, 2048), BF16),
    ((4, 2, 32, 256), BF16),
    ((4, 2, 32, 256), BF16),
    ((2, 4, 32, 256), BF16),
    ((2, 4, 32, 256), BF16),
    ((4, 32, 256), BF16),
    ((4, 32, 256), BF16),
    ((3, 32, 256), BF16),
    ((3, 32, 256), BF16),
    ((2, 32, 128), F32),
    ((32, 128), F32),
    ((32, 128), F32),
    ((2, 8, 32, 128), BF16),
    ((8, 32, 128), F32),
    ((8, 32, 128), BF16),
    ((8, 32, 128), BF16),
    ((7, 32, 128), BF16),
    ((2, 8, 32, 128), BF16),
    ((2, 128, 32), F32),
    ((16, 16, 512), BF16),
    ((2, 16, 16, 512), BF16),
    ((128, 2048), BF16),
    ((2, 2, 128, 512), BF16),
    ((2, 128, 512), F32),
    ((2, 128, 512), BF16),
    ((2, 16, 16, 256), BF16),
    ((2, 16, 16, 256), BF16),
    ((32, 2048), BF16),
    ((2, 8, 32, 128), BF16),
    ((8, 32, 128), F32),
    ((8, 32, 128), BF16),
    ((8, 32, 128), BF16),
    ((7, 32, 128), BF16),
]


def on_device(*args):
    (
        residual,
        mixer_gain,
        gate_proj,
        input_proj,
        write_proj,
        read_proj,
        step_proj,
        conv_weight,
        step_bias,
        log_rate,
        skip_gain,
        group_gain,
        ssm_state,
        conv_state,
        out_proj,
        ffn_gain,
        routes,
        route_weight,
        expert_gate,
        expert_up,
        expert_down,
        dense_gate,
        dense_up,
        dense_down,
        blend_weight,
    ) = args
    conv_t = jnp.transpose(conv_state, (1, 2, 0, 3))
    results = pl.pallas_call(
        kernel,
        out_shape=(
            pltpu.VMEM((32, 128), BF16),
            pltpu.VMEM((32, 2, 64, 128), F32),
            pltpu.VMEM((3, 3, 32, 128), BF16),
        ),
        in_specs=[HBM] * 25,
        out_specs=(VM, VM, VM),
        scratch_shapes=[pltpu.VMEM(s, d) for s, d in SCRATCH]
        + [
            pltpu.SemaphoreType.DMA((25,)),
            pltpu.SemaphoreType.DMA((12,)),
            pltpu.SemaphoreType.DMA((12,)),
            pltpu.SemaphoreType.DMA((6,)),
            pltpu.SemaphoreType.DMA((6,)),
            pltpu.SemaphoreType.DMA((21,)),
            pltpu.SemaphoreType.DMA((21,)),
            pltpu.SemaphoreType.DMA((5,)),
            pltpu.SemaphoreType.DMA((5,)),
            pltpu.SemaphoreType.DMA((15,)),
            pltpu.SemaphoreType.DMA((15,)),
            pltpu.SemaphoreType.DMA((16,)),
            pltpu.SemaphoreType.DMA((16,)),
            pltpu.SemaphoreType.DMA((30,)),
            pltpu.SemaphoreType.DMA((30,)),
            pltpu.SemaphoreType.DMA((2,)),
            pltpu.SemaphoreType.DMA((2,)),
            pltpu.SemaphoreType.REGULAR,
            pltpu.SemaphoreType.REGULAR,
        ],
        compiler_params=pltpu.CompilerParams(
            collective_id=0, has_side_effects=True, vmem_limit_bytes=64_400_000
        ),
    )(
        residual,
        mixer_gain.reshape(16, 128),
        gate_proj,
        input_proj,
        write_proj,
        read_proj,
        step_proj.T,
        jnp.transpose(conv_weight, (1, 0, 2)),
        step_bias.reshape(1, 32),
        log_rate.reshape(1, 32),
        skip_gain.reshape(1, 32),
        group_gain.reshape(16, 128),
        ssm_state,
        conv_t,
        out_proj,
        ffn_gain.reshape(16, 128),
        routes.T,
        route_weight.T,
        expert_gate,
        expert_up,
        expert_down,
        dense_gate,
        dense_up,
        dense_down,
        blend_weight.reshape(16, 128),
    )
    layer_out, new_state, new_conv = pl.pallas_call(
        write_out,
        out_shape=tuple(jax.ShapeDtypeStruct(r.shape, r.dtype) for r in results),
        in_specs=[ANY] * 3,
        out_specs=(HBM,) * 3,
        scratch_shapes=[pltpu.SemaphoreType.DMA((3,))],
        compiler_params=pltpu.CompilerParams(vmem_limit_bytes=1 << 20),
    )(*results)
    return layer_out, new_state, jnp.transpose(new_conv, (2, 0, 1, 3))


def solution(mesh):
    return jax.shard_map(
        on_device,
        mesh=mesh,
        in_specs=(
            P("ep", None),
            P(),
            P("ep", "tp"),
            P("ep", "tp"),
            P("ep", "tp"),
            P("ep", "tp"),
            P(),
            P(),
            P(),
            P(),
            P(),
            P(),
            P("ep", "tp", None, None),
            P("ep", None, None, "tp"),
            P("tp", None),
            P(),
            P("ep", None),
            P("ep", None),
            P("ep", None, "tp"),
            P("ep", None, "tp"),
            P("ep", "tp", None),
            P(None, "tp"),
            P(None, "tp"),
            P("tp", None),
            P(),
        ),
        out_specs=(P("ep", "tp"), P("ep", "tp", None, None), P("ep", None, None, "tp")),
        check_vma=False,
    )
```
